512 devices in a mesh: sp: 32 (over z, x), tp: 16 (over y, core).
Axes of the slice: x: 4, y: 8, z: 8, core: 2. Of those that a mesh axis runs over, the one named last changes fastest.
Arguments:
- mixer_out: bfloat16 [4096, 2048], P('sp'), may hold values from -6 to 6
- out_grad: bfloat16 [4096, 2048], P('sp'), may hold values from -2 to 2
- route_ids: int32 [4096, 2], P('sp'), may hold values from 0 to 31, all different within a row; in each aligned block of 128 rows (0 to 127, 128 to 255, ...) at most 16 rows name the same one
- route_weights: float32 [4096, 2], P('sp'), may hold values from 0.2 to 1.2
- gate_branch: bfloat16 [4096, 2048], P('sp', 'tp'), may hold values from -4 to 4
- states: float32 [4096, 2048], P('sp', 'tp'), may hold values from -6 to 6
- decay: float32 [4096, 2048], P('sp', 'tp'), may hold values from 0 to 1
- w_proj: bfloat16 [2048, 2048], P(None, 'tp'), may hold values from -0.125 to 0.125
- w_gate: bfloat16 [32, 2048, 2048], P('sp', 'tp'), may hold values from -0.125 to 0.125
- w_up: bfloat16 [32, 2048, 2048], P('sp', 'tp'), may hold values from -0.125 to 0.125
- w_down: bfloat16 [32, 2048, 2048], P('sp', 'tp'), may hold values from -0.125 to 0.125
Outputs:
- grad_w_gate: bfloat16 [32, 2048, 2048], P('sp', 'tp')
- grad_w_up: bfloat16 [32, 2048, 2048], P('sp', 'tp')
- grad_w_down: bfloat16 [32, 2048, 2048], P('sp', 'tp')
- grad_w_proj: float32 [2048, 2048], P('sp', 'tp')
- grad_branch: bfloat16 [4096, 2048], P('sp', 'tp')
- grad_drive: float32 [4096, 2048], P('sp', 'tp')
- grad_decay: float32 [4096, 2048], P('sp', 'tp')
The draws below stay inside these ranges and needn't reach their ends.
Inputs may be any that keep to these rules, and one draw needn't show every extreme that they name: `route_ids`: each row names 2 different experts. In the rows of one index of sp no expert is named more than 16 times, a bound that some block reaches.
All inputs are finite; a program needn't handle non-finite values.
Results may differ from the reference program's by a relative error of at most 0.02.
Values may be sent and summed in bfloat16 or wider, within the bound.
A program may use at most 64 MiB of HBM per device.

```python
import math
import jax
import jax.numpy as jnp
import numpy as np
from jax import lax

D = 2048
D_RNN = 2048
F = 2048
TOP = 2
TOK_DEV = 128
EXPERTS = 32
TOKENS = 4096
CAP = 16
N_SP = 32
N_TP = 16


def draw_decay(key, part):
    keys = jax.random.split(jax.random.fold_in(key, 17), 5)
    fast_share = 0.5
    fast = jax.random.uniform(keys[0], (D_RNN,), jnp.float32) < fast_share
    slow_rate = jax.random.uniform(keys[1], (D_RNN,), jnp.float32, 0.25, 0.8) / TOKENS
    fast_rate = jnp.exp(jax.random.uniform(keys[2], (D_RNN,), jnp.float32, jnp.log(0.01), jnp.log(1.0 / 30.0)))
    base_rate = jnp.where(fast, fast_rate, slow_rate)
    spans = TOKENS // 64
    factor = jnp.exp(jax.random.uniform(keys[3], (spans, 1), jnp.float32, jnp.log(0.4), jnp.log(1.6)))
    noise = jax.random.uniform(keys[4], (TOKENS, D_RNN), jnp.float32, 0.5, 1.5)
    return jnp.exp(-(base_rate[None, :] * jnp.repeat(factor, 64, axis=0) * noise))


def strengthened(array, own_key, source, target, shards_of, factor):
    owner, partner = [(jnp.arange(array.shape[dim]) // (array.shape[dim] // shards_of)).reshape([-1 if axis == dim else 1 for axis in range(array.ndim)]) for dim in (source, target)]
    chosen = jax.random.permutation(own_key, shards_of)[partner]
    strong = (owner == chosen) | (owner == (partner + shards_of // 2) % shards_of)
    return jnp.where(strong, factor * array, array)


def levels(stream_key, extent, cuts, smallest, largest):
    def one(axis_at, shards_of):
        steps = jax.random.uniform(jax.random.fold_in(jax.random.fold_in(stream_key, 6), axis_at), (shards_of,), jnp.float32, smallest / len(cuts), largest / len(cuts))
        return jnp.repeat(jnp.exp(steps), extent[axis_at] // shards_of).reshape((-1,) + (1,) * (len(extent) - axis_at - 1))

    loudness = one(*cuts[0])
    for cut in cuts[1:]:
        loudness = loudness * one(*cut)
    return loudness


def shared_out(key, own, number, rows, amount, top, most, skew):
    sequence = jax.random.permutation(key, amount)
    crowded, common = shares(amount, rows * top, most, skew, True), shares(amount, rows * top, most, skew, False)
    places = jnp.arange(amount)

    def named(lengths, turn):
        used = int((lengths > 0).sum())
        fixed = max(1, used // 4)
        passed = fixed + (places - fixed + turn * (used - fixed)) % max(1, amount - fixed)
        return jnp.zeros((amount,), jnp.int32).at[sequence[jnp.where(places < fixed, places, passed)]].set(jnp.asarray(lengths, jnp.int32))

    lengths = jnp.where(number % 4 == 0, named(crowded, number // 4), named(common, number - number // 4 - 1))
    mixed = jax.random.permutation(jax.random.fold_in(own, 3), amount)
    giver, receiver = mixed[0:amount // 2 * 2:2], mixed[1:amount // 2 * 2:2]
    margin = jnp.minimum(lengths[giver] - 1, most - lengths[receiver]) // 2
    margin = jnp.where((giver == sequence[0]) | (receiver == sequence[0]) | (lengths[receiver] == 0), 0, jnp.maximum(margin, 0))
    passed = jax.random.randint(jax.random.fold_in(own, 4), (amount // 2,), 0, 1 << 20) % (margin + 1)
    lengths = lengths.at[giver].add(-passed).at[receiver].add(passed)
    items = jnp.searchsorted(jnp.cumsum(lengths), jnp.arange(rows * top), side="right").astype(jnp.int32)
    listing = items.reshape(top, rows).T
    listing = listing[jax.random.permutation(jax.random.fold_in(own, 1), rows)]
    turn = jax.random.randint(jax.random.fold_in(own, 2), (rows, 1), 0, top)
    return jnp.take_along_axis(listing, (jnp.arange(top)[None, :] + turn) % top, axis=1)


def shares(count, total, limit, lean, full):
    weights = [(1 << 20) // math.isqrt(grade ** lean) + 1 for grade in range(1, count + 1)]
    largest = limit if full else min(limit, max(-(-total // count), total * weights[0] // sum(weights)))
    least = 1 if total - largest >= count - 1 else 0
    counts, rest = [largest] + [least] * (count - 1), total - largest - least * (count - 1)
    while rest > 0:
        movable = [i for i in range(1, count) if counts[i] < largest] or [i for i in range(1, count) if counts[i] < limit]
        mass, left = sum([weights[i] for i in movable]), rest
        for i in movable:
            extra = min(limit - counts[i], max(1, left * weights[i] // mass), rest)
            counts[i] = counts[i] + extra
            rest = rest - extra
    return np.array(counts)


def bell_draw(stream_key, dims, width, most, cuts=(), kind=jnp.bfloat16):
    entries = jax.random.normal(stream_key, dims, jnp.float32) * width
    if len(cuts) > 0:
        entries = levels(stream_key, dims, cuts, -0.22, 0.18) * entries
    return jnp.clip(entries, min=-most, max=most).astype(kind)


def noise_with(stream_key, shape, deviation, bound, shards, heavy, kind=jnp.bfloat16):
    entries = deviation * jax.random.normal(stream_key, shape, jnp.float32)
    if shards:
        entries = entries * levels(stream_key, shape, shards, -0.22, 0.18)
    return jnp.clip(strengthened(entries, jax.random.fold_in(stream_key, 3), *heavy), -bound, bound).astype(kind)


def setup_inputs(seed: int = 0) -> dict:
    key_list = jax.random.split(jax.random.key(seed), 12)
    mixer_out = bell_draw(key_list[0], (TOKENS, D), 1.0, 6.0, ((0, 32),))
    out_grad = noise_with(key_list[1], (TOKENS, D), 0.25, 2.0, ((0, 32),), (0, 1, 32, 2.75))
    route_ids_keys = jax.random.split(jax.random.fold_in(key_list[2], 1), TOKENS // TOK_DEV)
    route_ids_turns = jax.random.permutation(jax.random.fold_in(key_list[2], 3), TOKENS // TOK_DEV)
    route_ids = jax.vmap(lambda own, number: shared_out(jax.random.fold_in(key_list[2], 2), own, number, TOK_DEV, EXPERTS, TOP, CAP, 1))(route_ids_keys, route_ids_turns).reshape((TOKENS, TOP))
    route_weights = jnp.clip(0.2 + 1 * jax.random.uniform(key_list[3], (TOKENS, TOP), jnp.float32) ** levels(key_list[3], (TOKENS, TOP), ((0, 32),), -0.2, 0.2), 0.2, 1.2)
    gate_branch = bell_draw(key_list[4], (TOKENS, D_RNN), 0.5, 4.0, ((0, 32), (1, 16)))
    states = bell_draw(key_list[5], (TOKENS, D_RNN), 1.0, 6.0, ((0, 32), (1, 16)), jnp.float32)
    decay = draw_decay(jax.random.fold_in(key_list[11], 71), 0)
    w_proj = bell_draw(key_list[7], (D, D_RNN), D_RNN ** -0.5, 0.125, ((1, 16),))
    w_gate = bell_draw(key_list[8], (EXPERTS, F, D), D ** -0.5, 0.125, ((0, 32), (1, 16)))
    w_up = bell_draw(key_list[9], (EXPERTS, F, D), D ** -0.5, 0.125, ((0, 32), (1, 16)))
    w_down = bell_draw(key_list[10], (EXPERTS, F, D), F ** -0.5, 0.125, ((0, 32), (1, 16)))
    return dict(mixer_out=mixer_out, out_grad=out_grad, route_ids=route_ids, route_weights=route_weights, gate_branch=gate_branch, states=states, decay=decay, w_proj=w_proj, w_gate=w_gate, w_up=w_up, w_down=w_down)


def linear_combine(earlier, later):
    return earlier[0] * later[0], later[0] * earlier[1] + later[1]


def reference(mixer_out, out_grad, route_ids, route_weights, gate_branch, states, decay, w_proj, w_gate, w_up, w_down):
    routes = TOKENS * TOP
    flat_ids = route_ids.reshape(-1).astype(jnp.int32)
    onehot = (flat_ids[:, None] == jnp.arange(EXPERTS, dtype=jnp.int32)[None, :]).astype(jnp.int32)
    counted = jnp.cumsum(onehot.reshape(N_SP, TOK_DEV * TOP, EXPERTS), axis=1).reshape(routes, EXPERTS)
    position = (jnp.sum(counted * onehot, axis=1) - 1).astype(jnp.int32)
    block_id = (jnp.arange(routes, dtype=jnp.int32) // (TOK_DEV * TOP)).astype(jnp.int32)
    slot_index = ((flat_ids * N_SP + block_id) * CAP + position).astype(jnp.int32)
    table = jnp.full((EXPERTS * N_SP * CAP,), routes, jnp.int32).at[slot_index].set(jnp.arange(routes, dtype=jnp.int32))
    table = table.reshape(EXPERTS, N_SP * CAP)
    scaled = (route_weights[:, :, None].astype(jnp.float32) * out_grad[:, None, :].astype(jnp.float32)).astype(jnp.bfloat16)
    scaled_pad = jnp.concatenate([scaled.reshape(routes, D), jnp.zeros((1, D), jnp.bfloat16)], axis=0)
    token_pad = jnp.concatenate([mixer_out, jnp.zeros((1, D), jnp.bfloat16)], axis=0)

    def one_expert(carry, expert):
        slot_routes = table[expert]
        inputs = token_pad[slot_routes // TOP].astype(jnp.float32)
        cotangents = scaled_pad[slot_routes].astype(jnp.float32)
        weight_gate = w_gate[expert].astype(jnp.float32)
        weight_up = w_up[expert].astype(jnp.float32)
        weight_down = w_down[expert].astype(jnp.float32)
        gate_pre = jnp.dot(inputs, weight_gate.T, preferred_element_type=jnp.float32)
        up_pre = jnp.dot(inputs, weight_up.T, preferred_element_type=jnp.float32)
        sigmoid_gate = jax.nn.sigmoid(gate_pre)
        silu_gate = gate_pre * sigmoid_gate
        hidden = (silu_gate * up_pre).astype(jnp.bfloat16).astype(jnp.float32)
        hidden_grad = jnp.dot(cotangents, weight_down.T, preferred_element_type=jnp.float32)
        up_grad = (hidden_grad * silu_gate).astype(jnp.bfloat16).astype(jnp.float32)
        gate_grad = (hidden_grad * up_pre * sigmoid_gate * (1.0 + gate_pre * (1.0 - sigmoid_gate))).astype(jnp.bfloat16).astype(jnp.float32)
        grad_gate = jnp.dot(gate_grad.T, inputs, preferred_element_type=jnp.float32).astype(jnp.bfloat16)
        grad_up = jnp.dot(up_grad.T, inputs, preferred_element_type=jnp.float32).astype(jnp.bfloat16)
        grad_down = jnp.dot(hidden.T, cotangents, preferred_element_type=jnp.float32).astype(jnp.bfloat16)
        slots = slot_routes.shape[0]
        block_part = jnp.einsum("sbf,bfd->sbd", gate_grad.reshape(slots, N_TP, F // N_TP), weight_gate.reshape(N_TP, F // N_TP, D))
        block_part = block_part + jnp.einsum("sbf,bfd->sbd", up_grad.reshape(slots, N_TP, F // N_TP), weight_up.reshape(N_TP, F // N_TP, D))
        partial_value = jnp.sum(block_part.astype(jnp.bfloat16).astype(jnp.float32), axis=1)
        carry = carry.at[slot_routes].add(partial_value)
        return carry, (grad_gate, grad_up, grad_down)

    start_carry = jnp.zeros((routes + 1, D), jnp.float32)
    route_grad, stacked = lax.scan(one_expert, start_carry, jnp.arange(EXPERTS, dtype=jnp.int32))
    grad_w_gate, grad_w_up, grad_w_down = stacked
    routed_grad = jnp.sum(route_grad[:routes].reshape(TOKENS, TOP, D), axis=1)
    mid_grad = (out_grad.astype(jnp.float32) + routed_grad).astype(jnp.bfloat16)
    gated = (gate_branch.astype(jnp.float32) * states).astype(jnp.bfloat16)
    grad_w_proj = jnp.dot(mid_grad.T, gated, preferred_element_type=jnp.float32)
    act_grad = jnp.dot(mid_grad, w_proj, preferred_element_type=jnp.float32)
    grad_branch = (act_grad * states).astype(jnp.bfloat16)
    state_grad = act_grad * gate_branch.astype(jnp.float32)
    next_decay = jnp.concatenate([decay[1:], jnp.ones((1, D_RNN), jnp.float32)], axis=0)
    decay_prod, flipped = lax.associative_scan(linear_combine, (next_decay[::-1], state_grad[::-1]), axis=0)
    grad_drive = flipped[::-1]
    previous = jnp.concatenate([jnp.zeros((1, D_RNN), jnp.float32), states[:-1]], axis=0)
    grad_decay = grad_drive * previous
    return grad_w_gate, grad_w_up, grad_w_down, grad_w_proj, grad_branch, grad_drive, grad_decay
```

```python
import functools
import jax
import jax.numpy as jnp
from jax import lax
from jax.experimental import pallas as pl
from jax.experimental.pallas import tpu as pltpu
from jax.sharding import PartitionSpec as P

F32 = jnp.float32
BF16 = jnp.bfloat16
LANES = 128
MESH = pl.DeviceIdType.MESH


def dot(a, b, contract=((1,), (0,))):
    return lax.dot_general(a, b, (contract, ((), ())), preferred_element_type=F32)


def shift_up(a, k, fill):
    pad = jnp.full((k, a.shape[1]), fill, a.dtype)
    return jnp.concatenate([a[k:], pad], axis=0)


def kernel(
    sizes,
    ids, wts, mix, outg, gbr, st, dec, wp, wg, wu, wd,
    o_gate, o_up, o_down, o_proj, o_branch, o_drive, o_decay,
    onehot_s, disp, xc, acc_gu, acc_h, act_s, pbuf, precv, sbuf, rbuf, fin, ret, mid_all,
    gp_send, gp_recv, car_send, car_recv, prev_b,
    s1, r1, rs, ds, rr, ps, pr, cs, cr, fs, fr, ms, mf, mr, gs, gr, ks, kr, vs, vr,
):
    SP, TP, CAP = sizes
    Y = TP // 2
    H = Y // 2
    SH = SP // 2
    n = mix.shape[0]
    d_model = mix.shape[1]
    slots = SP * CAP
    me = lax.axis_index("sp")
    t = lax.axis_index("tp")
    y = t // 2
    core = t % 2
    partner = t + 1 - 2 * core
    right = (t + 2) % TP
    left = (t + TP - 2) % TP

    def chip(off):
        return (y + off + Y) % Y

    def remote(src, dst, send, recv, **device):
        return pltpu.make_async_remote_copy(
            src_ref=src, dst_ref=dst, send_sem=send, recv_sem=recv,
            device_id=device, device_id_type=MESH,
        )

    def each_peer(body):
        def step(i, carry):
            body((me + 1 + i) % SP)
            return carry

        lax.fori_loop(0, SP - 1, step, 0)

    barrier = pltpu.get_barrier_semaphore()
    each_peer(
        lambda p: pl.semaphore_signal(barrier, inc=1, device_id={"sp": p}, device_id_type=MESH)
    )
    for off in range(1, Y):
        pl.semaphore_signal(
            barrier, inc=1, device_id={"tp": (t + 2 * off) % TP}, device_id_type=MESH
        )
    pl.semaphore_signal(barrier, inc=1, device_id={"tp": partner}, device_id_type=MESH)

    own_cols = pl.ds(pl.multiple_of(t * LANES, LANES), LANES)
    expert_io = lax.broadcasted_iota(jnp.int32, (SP, n), 0)
    hots = [(expert_io == ids[k : k + 1, :]).astype(F32) for k in range(2)]
    earlier = (
        lax.broadcasted_iota(jnp.int32, (n, n), 0) < lax.broadcasted_iota(jnp.int32, (n, n), 1)
    ).astype(F32).astype(BF16)
    before = dot((hots[0] + hots[1]).astype(BF16), earlier)
    slot_io = lax.broadcasted_iota(jnp.int32, (slots, n), 0).astype(F32)
    picks = []
    for k in range(2):
        pos = jnp.sum(hots[k] * before, axis=0, keepdims=True)
        picks.append(slot_io == ids[k : k + 1, :].astype(F32) * float(CAP) + pos)
    onehot = (picks[0] | picks[1]).astype(F32).astype(BF16)
    onehot_s[...] = onehot
    weight = jnp.sum(
        jnp.where(picks[0], wts[0:1, :], 0.0) + jnp.where(picks[1], wts[1:2, :], 0.0),
        axis=1, keepdims=True,
    )
    x_slots = dot(onehot, mix[:, own_cols]).astype(BF16)
    c_slots = (weight * dot(onehot, outg[:, own_cols])).astype(BF16)
    disp[:, 0:CAP, :] = x_slots.reshape(SP, CAP, LANES)
    disp[:, CAP : 2 * CAP, :] = c_slots.reshape(SP, CAP, LANES)
    xc[t, me] = disp[me]

    pl.semaphore_wait(barrier, SP - 1 + Y)

    def dispatch(p):
        return remote(disp.at[p], xc.at[t, me], s1.at[p], r1.at[me], sp=p)

    each_peer(lambda p: dispatch(p).start())
    last_state = remote(
        st.at[pl.ds(n - 8, 8)], prev_b, vs.at[0], vr.at[0], sp=(me + 1) % SP
    )
    last_state.start()

    def arrived_1(half):
        def step(i, carry):
            b = half * SH + i

            @pl.when(b != me)
            def _():
                remote(disp.at[b], xc.at[t, b], s1.at[b], r1.at[b], sp=b).wait_recv()

            return carry

        lax.fori_loop(0, SH, step, 0)

    def half_of(src, h):
        return xc.at[src, pl.ds(h * SH, SH)]

    def ring(src, h, way, step):
        dev = right if way == 0 else left
        return remote(half_of(src, h), half_of(src, h), rs.at[way, h, step], rr.at[src, h], tp=dev)

    def across(src, h):
        return remote(
            half_of(src, h), half_of(src, h), ds.at[src // 2, h], rr.at[src, h], tp=partner
        )

    acc_gu[...] = jnp.zeros_like(acc_gu)
    acc_h[...] = jnp.zeros_like(acc_h)

    def pair_of(yy, part):
        lo, hi = (0, CAP) if part == 0 else (CAP, 2 * CAP)
        return jnp.concatenate(
            [xc[2 * yy + k, :, lo:hi, :].reshape(slots, LANES) for k in range(2)], axis=1
        )

    def cols_of(yy):
        return pl.ds(pl.multiple_of(yy * 2 * LANES, 2 * LANES), 2 * LANES)

    def forward(yy):
        other = 2 * yy + 1 - core
        for h in range(2):
            across(other, h).wait_recv()
        cols = cols_of(yy)
        w_in = jnp.concatenate([wg[:, cols], wu[:, cols]], axis=0)
        acc_gu[...] += dot(pair_of(yy, 0), w_in, ((1,), (1,)))
        acc_h[...] += dot(pair_of(yy, 1), wd[:, cols], ((1,), (1,)))

    for h in range(2):
        arrived_1(h)
        for way in range(2):
            ring(t, h, way, 0).start()
        across(t, h).start()

    for s in range(1, H + 1):
        for way, h in ((0, 0), (1, 1), (1, 0), (0, 1)):
            most = H if way == h else H - 1
            if s > most:
                continue
            src = 2 * chip(-s if way == 0 else s) + core
            ring(src, h, way, s - 1).wait_recv()
            if s < most:
                ring(src, h, way, s).start()
            across(src, h).start()
        forward(chip(s - 1))
        if s > 1:
            forward(chip(1 - s))
    forward(chip(H))

    gate = acc_gu[:, 0:LANES]
    up = acc_gu[:, LANES : 2 * LANES]
    hg = acc_h[...]
    sig = jax.nn.sigmoid(gate)
    silu = gate * sig
    hidden = (silu * up).astype(BF16)
    up_grad = (hg * silu).astype(BF16)
    gate_grad = (hg * up * sig * (1.0 + gate * (1.0 - sig))).astype(BF16)
    grads = jnp.concatenate([gate_grad, up_grad], axis=1)

    def partial(off):
        yy = chip(off)
        cols = cols_of(yy)
        value = dot(grads, jnp.concatenate([wg[:, cols], wu[:, cols]], axis=0)).astype(BF16)
        pbuf[yy, 0] = value[:, 0:LANES]
        pbuf[yy, 1] = value[:, LANES : 2 * LANES]
        swap(yy).start()

    def swap(yy):
        return remote(pbuf.at[yy, 1 - core], precv.at[yy], ps.at[yy], pr.at[yy], tp=partner)

    rows = slots // 2

    def own_sum(off, h):
        yy = chip(off)
        part = pl.ds(h * rows, rows)
        return pbuf[yy, core, part, :].astype(F32) + precv[yy, part, :].astype(F32)

    def chain(way, h, step):
        dev = right if way == 0 else left
        return remote(
            sbuf.at[way, h, step], rbuf.at[way, h, step],
            cs.at[way, h, step], cr.at[way, h, step], tp=dev,
        )

    flows = ((0, 0), (1, 1), (0, 1), (1, 0))

    def length(way, h):
        return H if way == h else H - 1

    def sign(way):
        return 1 if way == 0 else -1

    partial(H)
    partial(H - 1)
    partial(1 - H)
    swap(chip(H)).wait_recv()
    for way, h in flows[:2]:
        sbuf[way, h, 0] = own_sum(H, h).astype(BF16)
        chain(way, h, 0).start()
    for way, h in flows[2:]:
        off = sign(way) * (H - 1)
        swap(chip(off)).wait_recv()
        sbuf[way, h, 0] = own_sum(off, h).astype(BF16)
        chain(way, h, 0).start()
    for m in range(H - 2, 0, -1):
        partial(m)
        partial(-m)
    partial(0)
    for m in range(H - 2, 0, -1):
        swap(chip(m)).wait_recv()
        swap(chip(-m)).wait_recv()
    swap(chip(0)).wait_recv()

    grads_t = grads.T
    hidden_t = hidden.T

    def weight_grads(yy):
        cols = cols_of(yy)
        both = dot(grads_t, pair_of(yy, 0)).astype(BF16)
        o_gate[:, cols] = both[0:LANES]
        o_up[:, cols] = both[LANES : 2 * LANES]
        o_down[:, cols] = dot(hidden_t, pair_of(yy, 1)).astype(BF16)

    todo = list(range(Y))
    per_step = -(-Y // H)
    for s in range(1, H):
        for _ in range(per_step):
            if todo:
                weight_grads(todo.pop(0))
        for way, h in flows:
            most = length(way, h)
            if s >= most:
                continue
            off = sign(way) * (most - s)
            chain(way, h, s - 1).wait_recv()
            sbuf[way, h, s] = (rbuf[way, h, s - 1].astype(F32) + own_sum(off, h)).astype(BF16)
            chain(way, h, s).start()
    while todo:
        weight_grads(todo.pop(0))

    def give(p):
        return remote(fin.at[p], ret.at[me], fs.at[p], fr.at[me], sp=p)

    for h in range(2):
        total = own_sum(0, h)
        for way in range(2):
            step = length(way, h) - 1
            chain(way, h, step).wait_recv()
            total = total + rbuf[way, h, step].astype(F32)
        fin[pl.ds(h * SH, SH)] = total.astype(BF16).reshape(SH, CAP, LANES)

        def send_back(i, carry):
            b = h * SH + i

            @pl.when(b != me)
            def _():
                give(b).start()

            return carry

        lax.fori_loop(0, SH, send_back, 0)
    ret[me] = fin[me]

    onehot_t = onehot_s[...].T
    out_cols = outg[:, own_cols].astype(F32)
    gated = (gbr[...].astype(F32) * st[...]).astype(BF16)
    prod = shift_up(dec[...], 1, 1.0)
    shifts = [1 << k for k in range((n - 1).bit_length())]
    prods = []
    for k in shifts:
        prods.append(prod)
        prod = prod * shift_up(prod, k, 1.0)

    each_peer(lambda p: remote(fin.at[p], ret.at[p], fs.at[p], fr.at[p], sp=p).wait_recv())
    routed = dot(onehot_t, ret[...].reshape(slots, LANES))
    mid_all[t] = (out_cols + routed).astype(BF16)

    def share(off):
        return remote(
            mid_all.at[t], mid_all.at[t], ms.at[off], mr.at[t], tp=(t + 2 * off) % TP
        )

    def pass_mid(src):
        return remote(mid_all.at[src], mid_all.at[src], mf.at[src // 2], mr.at[src], tp=partner)

    order = [off for m in range(1, H) for off in (m, -m)] + [H]
    pass_mid(t).start()
    for off in order:
        share(off % Y).start()

    block = d_model // SP
    per_chip = 2 * LANES // block

    def give_proj(p):
        return remote(gp_send.at[p], gp_recv.at[me], gs.at[p], gr.at[me], sp=p)

    def project(yy):
        pass_mid(2 * yy + 1 - core).wait_recv()
        mid = jnp.concatenate([mid_all[2 * yy], mid_all[2 * yy + 1]], axis=1)
        part = dot(mid.T, gated).astype(BF16)
        for j in range(per_chip):
            owner = yy * per_chip + j
            gp_send[owner] = part[j * block : (j + 1) * block]

            @pl.when(owner != me)
            def _():
                give_proj(owner).start()

        return dot(mid, wp[cols_of(yy), :])

    act = None
    queue = [0]
    for off in order:
        src = 2 * chip(off) + core
        remote(mid_all.at[src], mid_all.at[src], mf.at[0], mr.at[src], tp=partner).wait_recv()
        pass_mid(src).start()
        ready = queue.pop(0)
        term = project(chip(ready))
        act = term if act is None else act + term
        queue.append(off)
    for off in queue:
        act = act + project(chip(off))
    gp_recv[me] = gp_send[me]

    states = st[...]
    o_branch[...] = (act * states).astype(BF16)
    grad = act * gbr[...].astype(F32)
    for k, a in zip(shifts, prods):
        grad = grad + a * shift_up(grad, k, 0.0)

    head = dec[0:1, :]
    car_send[0:1, :] = head * prod[0:1, :]
    car_send[1:2, :] = head * grad[0:1, :]

    def carry_to(p):
        return remote(car_send, car_recv.at[me], ks.at[p], kr.at[me], sp=p)

    each_peer(lambda p: carry_to(p).start())
    car_recv[me] = car_send[...]
    each_peer(lambda p: remote(car_send, car_recv.at[p], ks.at[p], kr.at[p], sp=p).wait_recv())

    def enter(i, value):
        b = SP - 1 - i
        pair = car_recv[b]
        later = jnp.where(b > me, 1.0, 0.0)
        return later * (pair[1:2, :] + pair[0:1, :] * value) + (1.0 - later) * value

    entering = lax.fori_loop(0, SP - 1, enter, jnp.zeros((1, LANES), F32))
    drive = grad + prod * entering
    o_drive[...] = drive
    last_state.wait_recv()
    first = jnp.where(me > 0, 1.0, 0.0) * prev_b[7:8, :]
    o_decay[...] = drive * jnp.concatenate([first, states[: n - 1]], axis=0)

    each_peer(lambda p: remote(gp_send.at[p], gp_recv.at[p], gs.at[p], gr.at[p], sp=p).wait_recv())

    def add(b, total):
        return total + gp_recv[b].astype(F32)

    o_proj[...] = lax.fori_loop(0, SP, add, jnp.zeros((block, LANES), F32))

    def drain(p):
        dispatch(p).wait_send()
        give(p).wait_send()
        give_proj(p).wait_send()
        carry_to(p).wait_send()

    each_peer(drain)
    last_state.wait_send()
    for way in range(2):
        for h in range(2):
            most = length(way, h)
            for s in range(most):
                ring(t, h, way, s).wait_send()
                chain(way, h, s).wait_send()
    for yy in range(Y):
        for h in range(2):
            across(2 * yy + core, h).wait_send()
        swap(yy).wait_send()
        pass_mid(2 * yy + core).wait_send()
    for off in range(1, Y):
        share(off).wait_send()


def local(
    mixer_out, out_grad, route_ids, route_weights, gate_branch, states, decay, w_proj,
    w_gate, w_up, w_down,
):
    n, d_model = mixer_out.shape
    SP = lax.axis_size("sp")
    TP = lax.axis_size("tp")
    Y, H = TP // 2, TP // 4
    CAP = min(n, 2 * route_ids.shape[1] * n // SP)
    slots = SP * CAP
    block = d_model // SP
    dma = pltpu.SemaphoreType.DMA
    big = jax.ShapeDtypeStruct((LANES, d_model), BF16)
    vmem = pl.BlockSpec(memory_space=pltpu.VMEM)
    outs = pl.pallas_call(
        functools.partial(kernel, (SP, TP, CAP)),
        out_shape=(
            big, big, big,
            jax.ShapeDtypeStruct((block, LANES), F32),
            jax.ShapeDtypeStruct((n, LANES), BF16),
            jax.ShapeDtypeStruct((n, LANES), F32),
            jax.ShapeDtypeStruct((n, LANES), F32),
        ),
        in_specs=[vmem] * 11,
        out_specs=(vmem,) * 7,
        scratch_shapes=[
            pltpu.VMEM((slots, n), BF16),
            pltpu.VMEM((SP, 2 * CAP, LANES), BF16),
            pltpu.VMEM((TP, SP, 2 * CAP, LANES), BF16),
            pltpu.VMEM((slots, 2 * LANES), F32),
            pltpu.VMEM((slots, LANES), F32),
            pltpu.VMEM((n, LANES), F32),
            pltpu.VMEM((Y, 2, slots, LANES), BF16),
            pltpu.VMEM((Y, slots, LANES), BF16),
            pltpu.VMEM((2, 2, H, slots // 2, LANES), BF16),
            pltpu.VMEM((2, 2, H, slots // 2, LANES), BF16),
            pltpu.VMEM((SP, CAP, LANES), BF16),
            pltpu.VMEM((SP, CAP, LANES), BF16),
            pltpu.VMEM((TP, n, LANES), BF16),
            pltpu.VMEM((SP, block, LANES), BF16),
            pltpu.VMEM((SP, block, LANES), BF16),
            pltpu.VMEM((2, LANES), F32),
            pltpu.VMEM((SP, 2, LANES), F32),
            pltpu.VMEM((8, LANES), F32),
            dma((SP,)), dma((SP,)),
            dma((2, 2, H)), dma((Y, 2)), dma((TP, 2)),
            dma((Y,)), dma((Y,)),
            dma((2, 2, H)), dma((2, 2, H)),
            dma((SP,)), dma((SP,)),
            dma((Y,)), dma((Y,)), dma((TP,)),
            dma((SP,)), dma((SP,)),
            dma((SP,)), dma((SP,)),
            dma((1,)), dma((1,)),
        ],
        compiler_params=pltpu.CompilerParams(
            collective_id=0, has_side_effects=True, vmem_limit_bytes=48 * 1024 * 1024
        ),
    )(
        route_ids.T, route_weights.T, mixer_out, out_grad, gate_branch, states, decay, w_proj,
        w_gate[0], w_up[0], w_down[0],
    )
    return (outs[0][None], outs[1][None], outs[2][None], *outs[3:])


def solution(mesh):
    placed = (
        P("sp", None),
        P("sp", None),
        P("sp", None),
        P("sp", None),
        P("sp", "tp"),
        P("sp", "tp"),
        P("sp", "tp"),
        P(None, "tp"),
        P("sp", "tp", None),
        P("sp", "tp", None),
        P("sp", "tp", None),
    )
    return jax.shard_map(
        local,
        mesh=mesh,
        in_specs=placed,
        out_specs=(
            P("sp", "tp", None),
            P("sp", "tp", None),
            P("sp", "tp", None),
            P("sp", "tp"),
            P("sp", "tp"),
            P("sp", "tp"),
            P("sp", "tp"),
        ),
        check_vma=False,
    )
```

```python
import functools
import jax
import jax.numpy as jnp
from jax import lax
from jax.experimental import pallas as pl
from jax.experimental.pallas import tpu as pltpu
from jax.sharding import PartitionSpec as P

F32 = jnp.float32
BF16 = jnp.bfloat16
LANES = 128
MESH = pl.DeviceIdType.MESH


def dot(a, b, contract=((1,), (0,))):
    return lax.dot_general(a, b, (contract, ((), ())), preferred_element_type=F32)


def shift_up(a, k, fill):
    pad = jnp.full((k, a.shape[1]), fill, a.dtype)
    return jnp.concatenate([a[k:], pad], axis=0)


def kernel(
    sizes,
    ids_h, wts_h, mix_h, outg_h, gbr_h, st_h, dec_h, wp_h, wg_h, wu_h, wd_h,
    o_gate, o_up, o_down, o_proj, o_branch, o_drive, o_decay,
    ids, wts, mix, outg, gbr, st, dec, wp, wg, wu, wd,
    onehot_s, disp, xc, acc_gu, acc_h, pbuf, precv, sbuf, rbuf, fin, ret, mid_all,
    gx_send, gx_recv, gz_send, gz_recv, car_send, car_recv, prev_b,
    ins, s1, r1, rs, ds, rr, ps, pr, cs, cr, fs, fr, ms, mf, mr, xs, xr, zs, zr, ks, kr, vs, vr,
):
    SP, X, TP, CAP = sizes
    Y = TP // 2
    H = Y // 2
    SH = SP // 2
    n = mix_h.shape[0]
    d_model = mix_h.shape[1]
    slots = SP * CAP
    me = lax.axis_index("sp")
    t = lax.axis_index("tp")
    y = t // 2
    core = t % 2
    partner = t + 1 - 2 * core
    right = (t + 2) % TP
    left = (t + TP - 2) % TP

    def chip(off):
        return (y + off + Y) % Y

    def remote(src, dst, send, recv, **device):
        return pltpu.make_async_remote_copy(
            src_ref=src, dst_ref=dst, send_sem=send, recv_sem=recv,
            device_id=device, device_id_type=MESH,
        )

    def each_peer(body):
        def step(i, carry):
            body((me + 1 + i) % SP)
            return carry

        lax.fori_loop(0, SP - 1, step, 0)

    barrier = pltpu.get_barrier_semaphore()
    each_peer(
        lambda p: pl.semaphore_signal(barrier, inc=1, device_id={"sp": p}, device_id_type=MESH)
    )
    for off in range(1, Y):
        pl.semaphore_signal(
            barrier, inc=1, device_id={"tp": (t + 2 * off) % TP}, device_id_type=MESH
        )
    pl.semaphore_signal(barrier, inc=1, device_id={"tp": partner}, device_id_type=MESH)

    own_cols = pl.ds(pl.multiple_of(t * LANES, LANES), LANES)
    fetch = [
        pltpu.make_async_copy(src, dst, ins.at[k])
        for k, (src, dst) in enumerate(
            (
                (ids_h, ids), (wts_h, wts), (mix_h.at[:, own_cols], mix),
                (outg_h.at[:, own_cols], outg), (st_h, st), (wg_h, wg), (wu_h, wu), (wd_h, wd),
                (gbr_h, gbr), (dec_h, dec), (wp_h, wp),
            )
        )
    ]
    for copy in fetch:
        copy.start()
    for copy in fetch[:4]:
        copy.wait()

    expert_io = lax.broadcasted_iota(jnp.int32, (SP, n), 0)
    hots = [(expert_io == ids[k : k + 1, :]).astype(F32) for k in range(2)]
    earlier = (
        lax.broadcasted_iota(jnp.int32, (n, n), 0) < lax.broadcasted_iota(jnp.int32, (n, n), 1)
    ).astype(F32).astype(BF16)
    before = dot((hots[0] + hots[1]).astype(BF16), earlier)
    slot_io = lax.broadcasted_iota(jnp.int32, (slots, n), 0).astype(F32)
    picks = []
    for k in range(2):
        pos = jnp.sum(hots[k] * before, axis=0, keepdims=True)
        picks.append(slot_io == ids[k : k + 1, :].astype(F32) * float(CAP) + pos)
    onehot = (picks[0] | picks[1]).astype(F32).astype(BF16)
    onehot_s[...] = onehot
    weight = jnp.sum(
        jnp.where(picks[0], wts[0:1, :], 0.0) + jnp.where(picks[1], wts[1:2, :], 0.0),
        axis=1, keepdims=True,
    )
    x_slots = dot(onehot, mix[...]).astype(BF16)
    c_slots = (weight * dot(onehot, outg[...])).astype(BF16)
    disp[:, 0:CAP, :] = x_slots.reshape(SP, CAP, LANES)
    disp[:, CAP : 2 * CAP, :] = c_slots.reshape(SP, CAP, LANES)
    xc[t, me] = disp[me]

    pl.semaphore_wait(barrier, SP - 1 + Y)

    def dispatch(p):
        return remote(disp.at[p], xc.at[t, me], s1.at[p], r1.at[me], sp=p)

    each_peer(lambda p: dispatch(p).start())
    for copy in fetch[4:]:
        copy.wait()
    last_state = remote(
        st.at[pl.ds(n - 8, 8)], prev_b, vs.at[0], vr.at[0], sp=(me + 1) % SP
    )
    last_state.start()

    def arrived_1(half):
        def step(i, carry):
            b = half * SH + i

            @pl.when(b != me)
            def _():
                remote(disp.at[b], xc.at[t, b], s1.at[b], r1.at[b], sp=b).wait_recv()

            return carry

        lax.fori_loop(0, SH, step, 0)

    def half_of(src, h):
        return xc.at[src, pl.ds(h * SH, SH)]

    def ring(src, h, way, step):
        dev = right if way == 0 else left
        return remote(half_of(src, h), half_of(src, h), rs.at[way, h, step], rr.at[src, h], tp=dev)

    def across(src, h):
        return remote(
            half_of(src, h), half_of(src, h), ds.at[src // 2, h], rr.at[src, h], tp=partner
        )

    acc_gu[...] = jnp.zeros_like(acc_gu)
    acc_h[...] = jnp.zeros_like(acc_h)

    def pair_of(yy, part):
        lo, hi = (0, CAP) if part == 0 else (CAP, 2 * CAP)
        return jnp.concatenate(
            [xc[2 * yy + k, :, lo:hi, :].reshape(slots, LANES) for k in range(2)], axis=1
        )

    def cols_of(yy):
        return pl.ds(pl.multiple_of(yy * 2 * LANES, 2 * LANES), 2 * LANES)

    def forward(yy):
        other = 2 * yy + 1 - core
        for h in range(2):
            across(other, h).wait_recv()
        cols = cols_of(yy)
        w_in = jnp.concatenate([wg[:, cols], wu[:, cols]], axis=0)
        acc_gu[...] += dot(pair_of(yy, 0), w_in, ((1,), (1,)))
        acc_h[...] += dot(pair_of(yy, 1), wd[:, cols], ((1,), (1,)))

    for h in range(2):
        arrived_1(h)
        for way in range(2):
            ring(t, h, way, 0).start()
        across(t, h).start()

    for s in range(1, H + 1):
        for way, h in ((0, 0), (1, 1), (1, 0), (0, 1)):
            most = H if way == h else H - 1
            if s > most:
                continue
            src = 2 * chip(-s if way == 0 else s) + core
            ring(src, h, way, s - 1).wait_recv()
            if s < most:
                ring(src, h, way, s).start()
            across(src, h).start()
        forward(chip(s - 1))
        if s > 1:
            forward(chip(1 - s))
    forward(chip(H))

    gate = acc_gu[:, 0:LANES]
    up = acc_gu[:, LANES : 2 * LANES]
    hg = acc_h[...]
    sig = jax.nn.sigmoid(gate)
    silu = gate * sig
    hidden = (silu * up).astype(BF16)
    up_grad = (hg * silu).astype(BF16)
    gate_grad = (hg * up * sig * (1.0 + gate * (1.0 - sig))).astype(BF16)
    grads = jnp.concatenate([gate_grad, up_grad], axis=1)

    def partial(off):
        yy = chip(off)
        cols = cols_of(yy)
        value = dot(grads, jnp.concatenate([wg[:, cols], wu[:, cols]], axis=0)).astype(BF16)
        pbuf[yy, 0] = value[:, 0:LANES]
        pbuf[yy, 1] = value[:, LANES : 2 * LANES]
        swap(yy).start()

    def swap(yy):
        return remote(pbuf.at[yy, 1 - core], precv.at[yy], ps.at[yy], pr.at[yy], tp=partner)

    rows = slots // 2

    def own_sum(off, h):
        yy = chip(off)
        part = pl.ds(h * rows, rows)
        return pbuf[yy, core, part, :].astype(F32) + precv[yy, part, :].astype(F32)

    def chain(way, h, step):
        dev = right if way == 0 else left
        return remote(
            sbuf.at[way, h, step], rbuf.at[way, h, step],
            cs.at[way, h, step], cr.at[way, h, step], tp=dev,
        )

    flows = ((0, 0), (1, 1), (0, 1), (1, 0))

    def length(way, h):
        return H if way == h else H - 1

    def sign(way):
        return 1 if way == 0 else -1

    partial(H)
    partial(H - 1)
    partial(1 - H)
    swap(chip(H)).wait_recv()
    for way, h in flows[:2]:
        sbuf[way, h, 0] = own_sum(H, h).astype(BF16)
        chain(way, h, 0).start()
    for way, h in flows[2:]:
        off = sign(way) * (H - 1)
        swap(chip(off)).wait_recv()
        sbuf[way, h, 0] = own_sum(off, h).astype(BF16)
        chain(way, h, 0).start()
    for m in range(H - 2, 0, -1):
        partial(m)
        partial(-m)
    partial(0)
    for m in range(H - 2, 0, -1):
        swap(chip(m)).wait_recv()
        swap(chip(-m)).wait_recv()
    swap(chip(0)).wait_recv()

    grads_t = grads.T
    hidden_t = hidden.T

    def weight_grads(yy):
        cols = cols_of(yy)
        both = dot(grads_t, pair_of(yy, 0)).astype(BF16)
        o_gate[:, cols] = both[0:LANES]
        o_up[:, cols] = both[LANES : 2 * LANES]
        o_down[:, cols] = dot(hidden_t, pair_of(yy, 1)).astype(BF16)

    todo = list(range(Y))
    per_step = -(-Y // H)
    for s in range(1, H):
        for _ in range(per_step):
            if todo:
                weight_grads(todo.pop(0))
        for way, h in flows:
            most = length(way, h)
            if s >= most:
                continue
            off = sign(way) * (most - s)
            chain(way, h, s - 1).wait_recv()
            sbuf[way, h, s] = (rbuf[way, h, s - 1].astype(F32) + own_sum(off, h)).astype(BF16)
            chain(way, h, s).start()
    while todo:
        weight_grads(todo.pop(0))

    def give(p):
        return remote(fin.at[p], ret.at[me], fs.at[p], fr.at[me], sp=p)

    for h in range(2):
        total = own_sum(0, h)
        for way in range(2):
            step = length(way, h) - 1
            chain(way, h, step).wait_recv()
            total = total + rbuf[way, h, step].astype(F32)
        fin[pl.ds(h * SH, SH)] = total.astype(BF16).reshape(SH, CAP, LANES)

        def send_back(i, carry):
            b = h * SH + i

            @pl.when(b != me)
            def _():
                give(b).start()

            return carry

        lax.fori_loop(0, SH, send_back, 0)
    ret[me] = fin[me]

    onehot_t = onehot_s[...].T
    out_cols = outg[...].astype(F32)
    gated = (gbr[...].astype(F32) * st[...]).astype(BF16)
    prod = shift_up(dec[...], 1, 1.0)
    shifts = [1 << k for k in range((n - 1).bit_length())]
    prods = []
    for k in shifts:
        prods.append(prod)
        prod = prod * shift_up(prod, k, 1.0)

    each_peer(lambda p: remote(fin.at[p], ret.at[p], fs.at[p], fr.at[p], sp=p).wait_recv())
    routed = dot(onehot_t, ret[...].reshape(slots, LANES))
    mid_all[t] = (out_cols + routed).astype(BF16)

    def share(off):
        return remote(
            mid_all.at[t], mid_all.at[t], ms.at[off], mr.at[t], tp=(t + 2 * off) % TP
        )

    def pass_mid(src):
        return remote(mid_all.at[src], mid_all.at[src], mf.at[src // 2], mr.at[src], tp=partner)

    order = [off for m in range(1, H) for off in (m, -m)] + [H]
    pass_mid(t).start()
    for off in order[::-1]:
        share(off % Y).start()

    block = d_model // SP
    z = me // X
    x = me % X

    def over_x(yy, j):
        return remote(
            gx_send.at[yy, j], gx_recv.at[yy, x], xs.at[yy, j], xr.at[yy, x], sp=z * X + j
        )

    def over_z(yy):
        return remote(gz_send.at[yy], gz_recv.at[z], zs.at[yy], zr.at[z], sp=yy * X + x)

    def x_peers(body):
        for j in range(1, X):
            body((x + j) % X)

    def project(yy):
        pass_mid(2 * yy + 1 - core).wait_recv()
        mid = jnp.concatenate([mid_all[2 * yy], mid_all[2 * yy + 1]], axis=1)
        part = dot(mid.T, gated).astype(BF16)
        gx_send[yy] = part.reshape(X, block, LANES)
        x_peers(lambda j: over_x(yy, j).start())
        return dot(mid, wp[cols_of(yy), :])

    def forward_proj(yy):
        total = gx_send[yy, x].astype(F32)
        for j in range(1, X):
            src = (x + j) % X
            remote(
                gx_send.at[yy, src], gx_recv.at[yy, src], xs.at[yy, src], xr.at[yy, src],
                sp=z * X + src,
            ).wait_recv()
            total = total + gx_recv[yy, src].astype(F32)
        gz_send[yy] = total.astype(BF16)

        @pl.when(yy != z)
        def _():
            over_z(yy).start()

    act = None
    queue = [0]
    behind = []
    for off in order:
        src = 2 * chip(off) + core
        remote(mid_all.at[src], mid_all.at[src], mf.at[0], mr.at[src], tp=partner).wait_recv()
        pass_mid(src).start()
        ready = queue.pop(0)
        term = project(chip(ready))
        act = term if act is None else act + term
        queue.append(off)
        behind.append(ready)
        if len(behind) > 2:
            forward_proj(chip(behind.pop(0)))
    for off in queue:
        act = act + project(chip(off))
        behind.append(off)

    states = st[...]
    o_branch[...] = (act * states).astype(BF16)
    grad = act * gbr[...].astype(F32)
    for k, a in zip(shifts, prods):
        grad = grad + a * shift_up(grad, k, 0.0)

    head = dec[0:1, :]
    car_send[0:1, :] = head * prod[0:1, :]
    car_send[1:2, :] = head * grad[0:1, :]

    def carry_to(p):
        return remote(car_send, car_recv.at[me], ks.at[p], kr.at[me], sp=p)

    each_peer(lambda p: carry_to(p).start())
    for off in behind:
        forward_proj(chip(off))
    car_recv[me] = car_send[...]
    each_peer(lambda p: remote(car_send, car_recv.at[p], ks.at[p], kr.at[p], sp=p).wait_recv())

    def enter(i, value):
        b = SP - 1 - i
        pair = car_recv[b]
        later = jnp.where(b > me, 1.0, 0.0)
        return later * (pair[1:2, :] + pair[0:1, :] * value) + (1.0 - later) * value

    entering = lax.fori_loop(0, SP - 1, enter, jnp.zeros((1, LANES), F32))
    drive = grad + prod * entering
    o_drive[...] = drive
    last_state.wait_recv()
    first = jnp.where(me > 0, 1.0, 0.0) * prev_b[7:8, :]
    o_decay[...] = drive * jnp.concatenate([first, states[: n - 1]], axis=0)

    def z_peers(body):
        def step(i, carry):
            body((z + 1 + i) % Y)
            return carry

        lax.fori_loop(0, Y - 1, step, 0)

    z_peers(
        lambda p: remote(
            gz_send.at[p], gz_recv.at[p], zs.at[p], zr.at[p], sp=p * X + x
        ).wait_recv()
    )
    total = gz_send[z].astype(F32)
    for i in range(1, Y):
        total = total + gz_recv[(z + i) % Y].astype(F32)
    o_proj[...] = total

    def drain(p):
        dispatch(p).wait_send()
        give(p).wait_send()
        carry_to(p).wait_send()

    each_peer(drain)
    last_state.wait_send()
    z_peers(lambda p: over_z(p).wait_send())
    for yy in range(Y):
        x_peers(lambda j: over_x(yy, j).wait_send())
    for way in range(2):
        for h in range(2):
            most = length(way, h)
            for s in range(most):
                ring(t, h, way, s).wait_send()
                chain(way, h, s).wait_send()
    for yy in range(Y):
        for h in range(2):
            across(2 * yy + core, h).wait_send()
        swap(yy).wait_send()
        pass_mid(2 * yy + core).wait_send()
    for off in range(1, Y):
        share(off).wait_send()


def store(*refs):
    count = len(refs) // 2
    copies = [
        pltpu.make_async_copy(refs[k], refs[count + k], refs[-1].at[k]) for k in range(count)
    ]
    for copy in copies:
        copy.start()
    for copy in copies:
        copy.wait()


def local(
    mixer_out, out_grad, route_ids, route_weights, gate_branch, states, decay, w_proj,
    w_gate, w_up, w_down,
):
    n, d_model = mixer_out.shape
    SP = lax.axis_size("sp")
    TP = lax.axis_size("tp")
    Y, H = TP // 2, TP // 4
    CAP = min(n, 2 * route_ids.shape[1] * n // SP)
    slots = SP * CAP
    X = SP // Y
    block = d_model // SP
    dma = pltpu.SemaphoreType.DMA
    big = jax.ShapeDtypeStruct((LANES, d_model), BF16)
    vmem = pl.BlockSpec(memory_space=pltpu.VMEM)
    outs = pl.pallas_call(
        functools.partial(kernel, (SP, SP // Y, TP, CAP)),
        out_shape=(
            big, big, big,
            jax.ShapeDtypeStruct((block, LANES), F32),
            jax.ShapeDtypeStruct((n, LANES), BF16),
            jax.ShapeDtypeStruct((n, LANES), F32),
            jax.ShapeDtypeStruct((n, LANES), F32),
        ),
        in_specs=[pl.BlockSpec(memory_space=pltpu.HBM)] * 11,
        out_specs=(vmem,) * 7,
        scratch_shapes=[
            pltpu.VMEM((2, n), jnp.int32),
            pltpu.VMEM((2, n), F32),
            pltpu.VMEM((n, LANES), BF16),
            pltpu.VMEM((n, LANES), BF16),
            pltpu.VMEM((n, LANES), BF16),
            pltpu.VMEM((n, LANES), F32),
            pltpu.VMEM((n, LANES), F32),
            pltpu.VMEM((d_model, LANES), BF16),
            pltpu.VMEM((LANES, d_model), BF16),
            pltpu.VMEM((LANES, d_model), BF16),
            pltpu.VMEM((LANES, d_model), BF16),
            pltpu.VMEM((slots, n), BF16),
            pltpu.VMEM((SP, 2 * CAP, LANES), BF16),
            pltpu.VMEM((TP, SP, 2 * CAP, LANES), BF16),
            pltpu.VMEM((slots, 2 * LANES), F32),
            pltpu.VMEM((slots, LANES), F32),
            pltpu.VMEM((Y, 2, slots, LANES), BF16),
            pltpu.VMEM((Y, slots, LANES), BF16),
            pltpu.VMEM((2, 2, H, slots // 2, LANES), BF16),
            pltpu.VMEM((2, 2, H, slots // 2, LANES), BF16),
            pltpu.VMEM((SP, CAP, LANES), BF16),
            pltpu.VMEM((SP, CAP, LANES), BF16),
            pltpu.VMEM((TP, n, LANES), BF16),
            pltpu.VMEM((Y, X, block, LANES), BF16),
            pltpu.VMEM((Y, X, block, LANES), BF16),
            pltpu.VMEM((Y, block, LANES), BF16),
            pltpu.VMEM((Y, block, LANES), BF16),
            pltpu.VMEM((2, LANES), F32),
            pltpu.VMEM((SP, 2, LANES), F32),
            pltpu.VMEM((8, LANES), F32),
            dma((11,)), dma((SP,)), dma((SP,)),
            dma((2, 2, H)), dma((Y, 2)), dma((TP, 2)),
            dma((Y,)), dma((Y,)),
            dma((2, 2, H)), dma((2, 2, H)),
            dma((SP,)), dma((SP,)),
            dma((Y,)), dma((Y,)), dma((TP,)),
            dma((Y, X)), dma((Y, X)), dma((Y,)), dma((Y,)),
            dma((SP,)), dma((SP,)),
            dma((1,)), dma((1,)),
        ],
        compiler_params=pltpu.CompilerParams(
            collective_id=0, has_side_effects=True, vmem_limit_bytes=48 * 1024 * 1024
        ),
    )(*(pltpu.with_memory_space_constraint(a, pltpu.HBM) for a in (
        route_ids.T, route_weights.T, mixer_out, out_grad, gate_branch, states, decay, w_proj,
        w_gate[0], w_up[0], w_down[0],
    )))
    outs = pl.pallas_call(
        store,
        out_shape=tuple(jax.ShapeDtypeStruct(o.shape, o.dtype) for o in outs),
        in_specs=[vmem] * len(outs),
        out_specs=(pl.BlockSpec(memory_space=pltpu.HBM),) * len(outs),
        scratch_shapes=[dma((len(outs),))], compiler_params=pltpu.CompilerParams(vmem_limit_bytes=4194304),
    )(*outs)
    return (outs[0][None], outs[1][None], outs[2][None], *outs[3:])


def solution(mesh):
    placed = (
        P("sp", None),
        P("sp", None),
        P("sp", None),
        P("sp", None),
        P("sp", "tp"),
        P("sp", "tp"),
        P("sp", "tp"),
        P(None, "tp"),
        P("sp", "tp", None),
        P("sp", "tp", None),
        P("sp", "tp", None),
    )
    return jax.shard_map(
        local,
        mesh=mesh,
        in_specs=placed,
        out_specs=(
            P("sp", "tp", None),
            P("sp", "tp", None),
            P("sp", "tp", None),
            P("sp", "tp"),
            P("sp", "tp"),
            P("sp", "tp"),
            P("sp", "tp"),
        ),
        check_vma=False,
    )
```

```python
import functools
import jax
import jax.numpy as jnp
from jax import lax
from jax.experimental import pallas as pl
from jax.experimental.pallas import tpu as pltpu
from jax.sharding import PartitionSpec as P

F32 = jnp.float32
BF16 = jnp.bfloat16
LANES = 128
MESH = pl.DeviceIdType.MESH


def dot(a, b, contract=((1,), (0,))):
    return lax.dot_general(a, b, (contract, ((), ())), preferred_element_type=F32)


def shift_up(a, k, fill):
    pad = jnp.full((k, a.shape[1]), fill, a.dtype)
    return jnp.concatenate([a[k:], pad], axis=0)


def kernel(
    sizes,
    ids_h, wts_h, mix_h, outg_h, gbr_h, st_h, dec_h, wp_h, wg_h, wu_h, wd_h,
    o_gate, o_up, o_down, o_proj, o_branch, o_drive, o_decay,
    ids, wts, mix, outg, gbr, st, dec, wp, wg, wu, wd,
    mixh, outh, onehot_s, weight_s, disp, near_send, xd, xc, acc_gu, acc_h, pbuf, precv, sbuf, rbuf, fin, ret, mid_all,
    gx_send, gx_recv, gz_send, gz_recv, car_send, car_recv, prev_b,
    ins, s1, r1, n1, n2, nr, rs, ds, rr, ps, pr, cs, cr, fs, fr, ms, mf, mr, xs, xr, zs, zr, ks, kr, vs, vr,
):
    SP, X, TP, CAP = sizes
    Y = TP // 2
    H = Y // 2
    Z = SP // X
    near = near_blocks(SP, X)
    far = SP - near
    SH = SP // 2
    FH = far // 2
    n = mix_h.shape[0]
    d_model = mix_h.shape[1]
    slots = SP * CAP
    me = lax.axis_index("sp")
    t = lax.axis_index("tp")
    y = t // 2
    core = t % 2
    partner = t + 1 - 2 * core
    right = (t + 2) % TP
    left = (t + TP - 2) % TP

    z = me // X
    x = me % X

    def chip(off):
        return (y + off + Y) % Y

    def moved(k, sign):
        zi = k // X
        dz = (zi + 1) // 2 * (2 * (zi % 2) - 1)
        return (z + sign * dz + Z) % Z * X + (x + sign * (k % X) + X) % X

    def target(k):
        return moved(k, 1)

    def source(k):
        return moved(k, -1)

    def each_block(lo, hi, body):
        def step(k, carry):
            body(k)
            return carry

        lax.fori_loop(lo, hi, step, 0)

    def remote(src, dst, send, recv, **device):
        return pltpu.make_async_remote_copy(
            src_ref=src, dst_ref=dst, send_sem=send, recv_sem=recv,
            device_id=device, device_id_type=MESH,
        )

    def each_peer(body):
        def step(i, carry):
            body((me + 1 + i) % SP)
            return carry

        lax.fori_loop(0, SP - 1, step, 0)

    barrier = pltpu.get_barrier_semaphore()
    each_peer(
        lambda p: pl.semaphore_signal(barrier, inc=1, device_id={"sp": p}, device_id_type=MESH)
    )
    for off in range(1, Y):
        pl.semaphore_signal(
            barrier, inc=1, device_id={"tp": (t + 2 * off) % TP}, device_id_type=MESH
        )
    pl.semaphore_signal(barrier, inc=1, device_id={"tp": partner}, device_id_type=MESH)

    own_cols = pl.ds(pl.multiple_of(t * LANES, LANES), LANES)
    width = d_model // 2
    half_cols = pl.ds(pl.multiple_of(core * width, width), width)
    fetch = [
        pltpu.make_async_copy(src, dst, ins.at[k])
        for k, (src, dst) in enumerate(
            (
                (ids_h, ids), (wts_h, wts), (mix_h.at[:, own_cols], mix),
                (outg_h.at[:, own_cols], outg), (st_h, st), (wg_h, wg), (wu_h, wu), (wd_h, wd),
                (gbr_h, gbr), (dec_h, dec), (wp_h, wp),
                (mix_h.at[:, half_cols], mixh), (outg_h.at[:, half_cols], outh),
            )
        )
    ]
    for copy in fetch:
        copy.start()
    for copy in fetch[:4]:
        copy.wait()

    expert_io = lax.broadcasted_iota(jnp.int32, (SP, n), 0)
    hots = [(expert_io == ids[k : k + 1, :]).astype(F32) for k in range(2)]
    earlier = (
        lax.broadcasted_iota(jnp.int32, (n, n), 0) < lax.broadcasted_iota(jnp.int32, (n, n), 1)
    ).astype(F32).astype(BF16)
    before = dot((hots[0] + hots[1]).astype(BF16), earlier)
    row = lax.broadcasted_iota(jnp.int32, (slots, n), 0)
    kk = row >> (CAP.bit_length() - 1)
    zi = kk >> (X.bit_length() - 1)
    zz = (z + Z + ((zi + 1) >> 1) * (2 * (zi & 1) - 1)) & (Z - 1)
    xx = (x + (kk & (X - 1))) & (X - 1)
    slot_io = ((zz * X + xx) * CAP + (row & (CAP - 1))).astype(F32)
    picks = []
    for k in range(2):
        pos = jnp.sum(hots[k] * before, axis=0, keepdims=True)
        picks.append(slot_io == ids[k : k + 1, :].astype(F32) * float(CAP) + pos)
    onehot = (picks[0] | picks[1]).astype(F32).astype(BF16)
    onehot_s[...] = onehot
    weight = jnp.sum(
        jnp.where(picks[0], wts[0:1, :], 0.0) + jnp.where(picks[1], wts[1:2, :], 0.0),
        axis=1, keepdims=True,
    )
    weight_s[...] = weight + jnp.zeros((slots, LANES), F32)
    first = near * CAP

    def into(ref, begin, lo, hi, mix_ref, out_ref):
        pick = onehot_s[lo:hi, :]
        shape = ((hi - lo) // CAP, CAP, mix_ref.shape[1])
        end = begin + (hi - lo) // CAP
        ref[begin:end, 0:CAP, :] = dot(pick, mix_ref[...]).astype(BF16).reshape(shape)
        scaled = weight_s[lo:hi, 0:1] * dot(pick, out_ref[...])
        ref[begin:end, CAP : 2 * CAP, :] = scaled.astype(BF16).reshape(shape)

    into(disp, 0, first, slots, mix, outg)

    pl.semaphore_wait(barrier, SP - 1 + Y)

    def dispatch(k):
        return remote(disp.at[k], xc.at[t, k], s1.at[k], r1.at[k], sp=target(near + k))

    def dispatch_near(k):
        return remote(near_send.at[k], xd.at[core, k], n1.at[k], nr.at[core, k], sp=target(k))

    def across_near(k, half):
        return remote(xd.at[half, k], xd.at[half, k], n2.at[k], nr.at[half, k], tp=partner)

    each_block(0, far, lambda k: dispatch(k).start())
    for copy in fetch[11:]:
        copy.wait()
    into(near_send, 0, 0, first, mixh, outh)
    each_block(1, near, lambda k: dispatch_near(k).start())
    xd[core, 0] = near_send[0]
    across_near(0, core).start()
    for copy in fetch[4:11]:
        copy.wait()
    last_state = remote(
        st.at[pl.ds(n - 8, 8)], prev_b, vs.at[0], vr.at[0], sp=(me + 1) % SP
    )
    last_state.start()

    def arrived_1(half):
        each_block(half * FH, half * FH + FH, lambda k: dispatch(k).wait_recv())

    def half_of(src, h):
        return xc.at[src, pl.ds(h * FH, FH)]

    def ring(src, h, way, step):
        dev = right if way == 0 else left
        return remote(half_of(src, h), half_of(src, h), rs.at[way, h, step], rr.at[src, h], tp=dev)

    def across(src, h):
        return remote(
            half_of(src, h), half_of(src, h), ds.at[src // 2, h], rr.at[src, h], tp=partner
        )

    acc_gu[...] = jnp.zeros_like(acc_gu)
    acc_h[...] = jnp.zeros_like(acc_h)

    def span(part):
        return (0, CAP) if part == 0 else (CAP, 2 * CAP)

    def pair_of(yy, part):
        lo, hi = span(part)
        return jnp.concatenate(
            [xc[2 * yy + k, :, lo:hi, :].reshape(far * CAP, LANES) for k in range(2)], axis=1
        )

    def near_rows(yy, part):
        lo, hi = span(part)
        at = yy % H * 2 * LANES
        return xd[yy // H, :, lo:hi, at : at + 2 * LANES].reshape(first, 2 * LANES)

    def forward_near(half):
        cols = pl.ds(pl.multiple_of(half * width, width), width)
        w_in = jnp.concatenate([wg[:, cols], wu[:, cols]], axis=0)
        rows_x = xd[half, :, 0:CAP, :].reshape(first, width)
        rows_c = xd[half, :, CAP : 2 * CAP, :].reshape(first, width)
        acc_gu[0:first] += dot(rows_x, w_in, ((1,), (1,)))
        acc_h[0:first] += dot(rows_c, wd[:, cols], ((1,), (1,)))

    def cols_of(yy):
        return pl.ds(pl.multiple_of(yy * 2 * LANES, 2 * LANES), 2 * LANES)

    def forward(yy):
        other = 2 * yy + 1 - core
        for h in range(2):
            across(other, h).wait_recv()
        cols = cols_of(yy)
        w_in = jnp.concatenate([wg[:, cols], wu[:, cols]], axis=0)
        acc_gu[first:slots] += dot(pair_of(yy, 0), w_in, ((1,), (1,)))
        acc_h[first:slots] += dot(pair_of(yy, 1), wd[:, cols], ((1,), (1,)))

    for h in range(2):
        arrived_1(h)
        for way in range(2):
            ring(t, h, way, 0).start()
        across(t, h).start()

    for s in range(1, H + 1):
        for way, h in ((0, 0), (1, 1), (1, 0), (0, 1)):
            most = H if way == h else H - 1
            if s > most:
                continue
            src = 2 * chip(-s if way == 0 else s) + core
            ring(src, h, way, s - 1).wait_recv()
            if s < most:
                ring(src, h, way, s).start()
            across(src, h).start()
        if s == H // 2:

            def pass_near(k):
                dispatch_near(k).wait_recv()
                across_near(k, core).start()

            each_block(1, near, pass_near)
        forward(chip(s - 1))
        if s > 1:
            forward(chip(1 - s))
    forward_near(core)
    each_block(0, near, lambda k: across_near(k, 1 - core).wait_recv())
    forward_near(1 - core)
    forward(chip(H))

    gate = acc_gu[:, 0:LANES]
    up = acc_gu[:, LANES : 2 * LANES]
    hg = acc_h[...]
    sig = jax.nn.sigmoid(gate)
    silu = gate * sig
    hidden = (silu * up).astype(BF16)
    up_grad = (hg * silu).astype(BF16)
    gate_grad = (hg * up * sig * (1.0 + gate * (1.0 - sig))).astype(BF16)
    grads = jnp.concatenate([gate_grad, up_grad], axis=1)

    def partial(off):
        yy = chip(off)
        cols = cols_of(yy)
        value = dot(grads, jnp.concatenate([wg[:, cols], wu[:, cols]], axis=0)).astype(BF16)
        pbuf[yy, 0] = value[:, 0:LANES]
        pbuf[yy, 1] = value[:, LANES : 2 * LANES]
        swap(yy).start()

    def swap(yy):
        return remote(pbuf.at[yy, 1 - core], precv.at[yy], ps.at[yy], pr.at[yy], tp=partner)

    rows = slots // 2

    def own_sum(off, h):
        yy = chip(off)
        part = pl.ds(h * rows, rows)
        return pbuf[yy, core, part, :].astype(F32) + precv[yy, part, :].astype(F32)

    def chain(way, h, step):
        dev = right if way == 0 else left
        return remote(
            sbuf.at[way, h, step], rbuf.at[way, h, step],
            cs.at[way, h, step], cr.at[way, h, step], tp=dev,
        )

    flows = ((0, 0), (1, 1), (0, 1), (1, 0))

    def length(way, h):
        return H if way == h else H - 1

    def sign(way):
        return 1 if way == 0 else -1

    partial(H)
    partial(H - 1)
    partial(1 - H)
    swap(chip(H)).wait_recv()
    for way, h in flows[:2]:
        sbuf[way, h, 0] = own_sum(H, h).astype(BF16)
        chain(way, h, 0).start()
    for way, h in flows[2:]:
        off = sign(way) * (H - 1)
        swap(chip(off)).wait_recv()
        sbuf[way, h, 0] = own_sum(off, h).astype(BF16)
        chain(way, h, 0).start()
    for m in range(H - 2, 0, -1):
        partial(m)
        partial(-m)
    partial(0)
    for m in range(H - 2, 0, -1):
        swap(chip(m)).wait_recv()
        swap(chip(-m)).wait_recv()
    swap(chip(0)).wait_recv()

    grads_t = grads.T
    hidden_t = hidden.T

    def all_rows(yy, part):
        return jnp.concatenate([near_rows(yy, part), pair_of(yy, part)], axis=0)

    def weight_grads(yy):
        cols = cols_of(yy)
        both = dot(grads_t, all_rows(yy, 0)).astype(BF16)
        o_gate[:, cols] = both[0:LANES]
        o_up[:, cols] = both[LANES : 2 * LANES]
        o_down[:, cols] = dot(hidden_t, all_rows(yy, 1)).astype(BF16)

    todo = list(range(Y))
    per_step = -(-Y // H)
    for s in range(1, H):
        for _ in range(per_step):
            if todo:
                weight_grads(todo.pop(0))
        for way, h in flows:
            most = length(way, h)
            if s >= most:
                continue
            off = sign(way) * (most - s)
            chain(way, h, s - 1).wait_recv()
            sbuf[way, h, s] = (rbuf[way, h, s - 1].astype(F32) + own_sum(off, h)).astype(BF16)
            chain(way, h, s).start()
    while todo:
        weight_grads(todo.pop(0))

    def give(k):
        return remote(fin.at[k], ret.at[k], fs.at[k], fr.at[k], sp=source(k))

    for h in range(2):
        total = own_sum(0, h)
        for way in range(2):
            step = length(way, h) - 1
            chain(way, h, step).wait_recv()
            total = total + rbuf[way, h, step].astype(F32)
        fin[pl.ds(h * SH, SH)] = total.astype(BF16).reshape(SH, CAP, LANES)

        each_block(max(1, h * SH), (h + 1) * SH, lambda k: give(k).start())
    ret[0] = fin[0]

    onehot_t = onehot_s[...].T
    out_cols = outg[...].astype(F32)
    gated = (gbr[...].astype(F32) * st[...]).astype(BF16)
    prod = shift_up(dec[...], 1, 1.0)
    shifts = [1 << k for k in range((n - 1).bit_length())]
    prods = []
    for k in shifts:
        prods.append(prod)
        prod = prod * shift_up(prod, k, 1.0)

    each_block(1, SP, lambda k: give(k).wait_recv())
    routed = dot(onehot_t, ret[...].reshape(slots, LANES))
    mid_all[t] = (out_cols + routed).astype(BF16)

    def share(off):
        return remote(
            mid_all.at[t], mid_all.at[t], ms.at[off], mr.at[t], tp=(t + 2 * off) % TP
        )

    def pass_mid(src):
        return remote(mid_all.at[src], mid_all.at[src], mf.at[src // 2], mr.at[src], tp=partner)

    order = [off for m in range(1, H) for off in (m, -m)] + [H]
    pass_mid(t).start()
    for off in order[::-1]:
        share(off % Y).start()

    block = d_model // SP

    def over_x(yy, j):
        return remote(
            gx_send.at[yy, j], gx_recv.at[yy, x], xs.at[yy, j], xr.at[yy, x], sp=z * X + j
        )

    def over_z(yy):
        return remote(gz_send.at[yy], gz_recv.at[z], zs.at[yy], zr.at[z], sp=yy * X + x)

    def x_peers(body):
        for j in range(1, X):
            body((x + j) % X)

    def project(yy):
        pass_mid(2 * yy + 1 - core).wait_recv()
        mid = jnp.concatenate([mid_all[2 * yy], mid_all[2 * yy + 1]], axis=1)
        part = dot(mid.T, gated).astype(BF16)
        gx_send[yy] = part.reshape(X, block, LANES)
        x_peers(lambda j: over_x(yy, j).start())
        return dot(mid, wp[cols_of(yy), :])

    def forward_proj(yy):
        total = gx_send[yy, x].astype(F32)
        for j in range(1, X):
            src = (x + j) % X
            remote(
                gx_send.at[yy, src], gx_recv.at[yy, src], xs.at[yy, src], xr.at[yy, src],
                sp=z * X + src,
            ).wait_recv()
            total = total + gx_recv[yy, src].astype(F32)
        gz_send[yy] = total.astype(BF16)

        @pl.when(yy != z)
        def _():
            over_z(yy).start()

    act = None
    queue = [0]
    behind = []
    for off in order:
        src = 2 * chip(off) + core
        remote(mid_all.at[src], mid_all.at[src], mf.at[0], mr.at[src], tp=partner).wait_recv()
        pass_mid(src).start()
        ready = queue.pop(0)
        term = project(chip(ready))
        act = term if act is None else act + term
        queue.append(off)
        behind.append(ready)
        if len(behind) > 2:
            forward_proj(chip(behind.pop(0)))
    for off in queue:
        act = act + project(chip(off))
        behind.append(off)

    states = st[...]
    o_branch[...] = (act * states).astype(BF16)
    grad = act * gbr[...].astype(F32)
    for k, a in zip(shifts, prods):
        grad = grad + a * shift_up(grad, k, 0.0)

    head = dec[0:1, :]
    car_send[0:1, :] = head * prod[0:1, :]
    car_send[1:2, :] = head * grad[0:1, :]

    def carry_to(p):
        return remote(car_send, car_recv.at[me], ks.at[p], kr.at[me], sp=p)

    each_peer(lambda p: carry_to(p).start())
    for off in behind:
        forward_proj(chip(off))
    car_recv[me] = car_send[...]
    each_peer(lambda p: remote(car_send, car_recv.at[p], ks.at[p], kr.at[p], sp=p).wait_recv())

    def enter(i, value):
        b = SP - 1 - i
        pair = car_recv[b]
        later = jnp.where(b > me, 1.0, 0.0)
        return later * (pair[1:2, :] + pair[0:1, :] * value) + (1.0 - later) * value

    entering = lax.fori_loop(0, SP - 1, enter, jnp.zeros((1, LANES), F32))
    drive = grad + prod * entering
    o_drive[...] = drive
    last_state.wait_recv()
    prior = jnp.where(me > 0, 1.0, 0.0) * prev_b[7:8, :]
    o_decay[...] = drive * jnp.concatenate([prior, states[: n - 1]], axis=0)

    def z_peers(body):
        def step(i, carry):
            body((z + 1 + i) % Y)
            return carry

        lax.fori_loop(0, Y - 1, step, 0)

    z_peers(
        lambda p: remote(
            gz_send.at[p], gz_recv.at[p], zs.at[p], zr.at[p], sp=p * X + x
        ).wait_recv()
    )
    total = gz_send[z].astype(F32)
    for i in range(1, Y):
        total = total + gz_recv[(z + i) % Y].astype(F32)
    o_proj[...] = total

    def drain(p):
        carry_to(p).wait_send()

    each_peer(drain)
    each_block(0, far, lambda k: dispatch(k).wait_send())
    each_block(1, near, lambda k: dispatch_near(k).wait_send())
    each_block(0, near, lambda k: across_near(k, core).wait_send())
    each_block(1, SP, lambda k: give(k).wait_send())
    last_state.wait_send()
    z_peers(lambda p: over_z(p).wait_send())
    for yy in range(Y):
        x_peers(lambda j: over_x(yy, j).wait_send())
    for way in range(2):
        for h in range(2):
            most = length(way, h)
            for s in range(most):
                ring(t, h, way, s).wait_send()
                chain(way, h, s).wait_send()
    for yy in range(Y):
        for h in range(2):
            across(2 * yy + core, h).wait_send()
        swap(yy).wait_send()
        pass_mid(2 * yy + core).wait_send()
    for off in range(1, Y):
        share(off).wait_send()


def near_blocks(SP, X):
    return 3 * X


def store(*refs):
    count = len(refs) // 2
    copies = [
        pltpu.make_async_copy(refs[k], refs[count + k], refs[-1].at[k]) for k in range(count)
    ]
    for copy in copies:
        copy.start()
    for copy in copies:
        copy.wait()


def local(
    mixer_out, out_grad, route_ids, route_weights, gate_branch, states, decay, w_proj,
    w_gate, w_up, w_down,
):
    n, d_model = mixer_out.shape
    SP = lax.axis_size("sp")
    TP = lax.axis_size("tp")
    Y, H = TP // 2, TP // 4
    CAP = min(n, 2 * route_ids.shape[1] * n // SP)
    slots = SP * CAP
    X = SP // Y
    near = near_blocks(SP, X)
    far = SP - near
    block = d_model // SP
    dma = pltpu.SemaphoreType.DMA
    big = jax.ShapeDtypeStruct((LANES, d_model), BF16)
    vmem = pl.BlockSpec(memory_space=pltpu.VMEM)
    outs = pl.pallas_call(
        functools.partial(kernel, (SP, SP // Y, TP, CAP)),
        out_shape=(
            big, big, big,
            jax.ShapeDtypeStruct((block, LANES), F32),
            jax.ShapeDtypeStruct((n, LANES), BF16),
            jax.ShapeDtypeStruct((n, LANES), F32),
            jax.ShapeDtypeStruct((n, LANES), F32),
        ),
        in_specs=[pl.BlockSpec(memory_space=pltpu.HBM)] * 11,
        out_specs=(vmem,) * 7,
        scratch_shapes=[
            pltpu.VMEM((2, n), jnp.int32),
            pltpu.VMEM((2, n), F32),
            pltpu.VMEM((n, LANES), BF16),
            pltpu.VMEM((n, LANES), BF16),
            pltpu.VMEM((n, LANES), BF16),
            pltpu.VMEM((n, LANES), F32),
            pltpu.VMEM((n, LANES), F32),
            pltpu.VMEM((d_model, LANES), BF16),
            pltpu.VMEM((LANES, d_model), BF16),
            pltpu.VMEM((LANES, d_model), BF16),
            pltpu.VMEM((LANES, d_model), BF16),
            pltpu.VMEM((n, d_model // 2), BF16),
            pltpu.VMEM((n, d_model // 2), BF16),
            pltpu.VMEM((slots, n), BF16),
            pltpu.VMEM((slots, LANES), F32),
            pltpu.VMEM((far, 2 * CAP, LANES), BF16),
            pltpu.VMEM((near, 2 * CAP, d_model // 2), BF16),
            pltpu.VMEM((2, near, 2 * CAP, d_model // 2), BF16),
            pltpu.VMEM((TP, far, 2 * CAP, LANES), BF16),
            pltpu.VMEM((slots, 2 * LANES), F32),
            pltpu.VMEM((slots, LANES), F32),
            pltpu.VMEM((Y, 2, slots, LANES), BF16),
            pltpu.VMEM((Y, slots, LANES), BF16),
            pltpu.VMEM((2, 2, H, slots // 2, LANES), BF16),
            pltpu.VMEM((2, 2, H, slots // 2, LANES), BF16),
            pltpu.VMEM((SP, CAP, LANES), BF16),
            pltpu.VMEM((SP, CAP, LANES), BF16),
            pltpu.VMEM((TP, n, LANES), BF16),
            pltpu.VMEM((Y, X, block, LANES), BF16),
            pltpu.VMEM((Y, X, block, LANES), BF16),
            pltpu.VMEM((Y, block, LANES), BF16),
            pltpu.VMEM((Y, block, LANES), BF16),
            pltpu.VMEM((2, LANES), F32),
            pltpu.VMEM((SP, 2, LANES), F32),
            pltpu.VMEM((8, LANES), F32),
            dma((13,)), dma((far,)), dma((far,)), dma((near,)), dma((near,)), dma((2, near)),
            dma((2, 2, H)), dma((Y, 2)), dma((TP, 2)),
            dma((Y,)), dma((Y,)),
            dma((2, 2, H)), dma((2, 2, H)),
            dma((SP,)), dma((SP,)),
            dma((Y,)), dma((Y,)), dma((TP,)),
            dma((Y, X)), dma((Y, X)), dma((Y,)), dma((Y,)),
            dma((SP,)), dma((SP,)),
            dma((1,)), dma((1,)),
        ],
        compiler_params=pltpu.CompilerParams(
            collective_id=0, has_side_effects=True, vmem_limit_bytes=48 * 1024 * 1024
        ),
    )(*(pltpu.with_memory_space_constraint(a, pltpu.HBM) for a in (
        route_ids.T, route_weights.T, mixer_out, out_grad, gate_branch, states, decay, w_proj,
        w_gate[0], w_up[0], w_down[0],
    )))
    outs = pl.pallas_call(
        store,
        out_shape=tuple(jax.ShapeDtypeStruct(o.shape, o.dtype) for o in outs),
        in_specs=[vmem] * len(outs),
        out_specs=(pl.BlockSpec(memory_space=pltpu.HBM),) * len(outs),
        scratch_shapes=[dma((len(outs),))], compiler_params=pltpu.CompilerParams(vmem_limit_bytes=4194304),
    )(*outs)
    return (outs[0][None], outs[1][None], outs[2][None], *outs[3:])


def solution(mesh):
    placed = (
        P("sp", None),
        P("sp", None),
        P("sp", None),
        P("sp", None),
        P("sp", "tp"),
        P("sp", "tp"),
        P("sp", "tp"),
        P(None, "tp"),
        P("sp", "tp", None),
        P("sp", "tp", None),
        P("sp", "tp", None),
    )
    return jax.shard_map(
        local,
        mesh=mesh,
        in_specs=placed,
        out_specs=(
            P("sp", "tp", None),
            P("sp", "tp", None),
            P("sp", "tp", None),
            P("sp", "tp"),
            P("sp", "tp"),
            P("sp", "tp"),
            P("sp", "tp"),
        ),
        check_vma=False,
    )
```

```python
import functools
import jax
import jax.numpy as jnp
from jax import lax
from jax.experimental import pallas as pl
from jax.experimental.pallas import tpu as pltpu
from jax.sharding import PartitionSpec as P

F32 = jnp.float32
BF16 = jnp.bfloat16
LANES = 128
MESH = pl.DeviceIdType.MESH


def dot(a, b, contract=((1,), (0,))):
    return lax.dot_general(a, b, (contract, ((), ())), preferred_element_type=F32)


def shift_up(a, k, fill):
    pad = jnp.full((k, a.shape[1]), fill, a.dtype)
    return jnp.concatenate([a[k:], pad], axis=0)


def kernel(
    sizes,
    ids_h, wts_h, mix_h, outg_h, gbr_h, st_h, dec_h, wp_h, wg_h, wu_h, wd_h,
    o_gate, o_up, o_down, o_proj, o_branch, o_drive, o_decay,
    ids, wts, mix, outg, gbr, st, dec, wp, wg, wu, wd,
    mixh, outh, onehot_s, weight_s, disp, near_send, xd, xc, acc_gu, acc_h, pbuf, precv, sbuf, rbuf, fin, ret, mid_all,
    gx_send, gx_recv, gz_send, gz_recv, car_send, car_recv, prev_b,
    ins, s1, r1, n1, n2, nr, rs, ds, rr, ps, pr, cs, cr, fs, fr, ms, mf, mr, xs, xr, zs, zr, ks, kr, vs, vr,
):
    SP, X, TP, CAP = sizes
    Y = TP // 2
    H = Y // 2
    Z = SP // X
    near = near_blocks(SP, X)
    far = SP - near
    groups = ring_groups(far, X)
    quarter = SP // 4
    n = mix_h.shape[0]
    d_model = mix_h.shape[1]
    slots = SP * CAP
    me = lax.axis_index("sp")
    t = lax.axis_index("tp")
    y = t // 2
    core = t % 2
    partner = t + 1 - 2 * core
    right = (t + 2) % TP
    left = (t + TP - 2) % TP

    z = me // X
    x = me % X

    def chip(off):
        return (y + off + Y) % Y

    def moved(k, sign):
        zi = k // X
        dz = (zi + 1) // 2 * (2 * (zi % 2) - 1)
        return (z + sign * dz + Z) % Z * X + (x + sign * (k % X) + X) % X

    def target(k):
        return moved(k, 1)

    def source(k):
        return moved(k, -1)

    def each_block(lo, hi, body):
        def step(k, carry):
            body(k)
            return carry

        lax.fori_loop(lo, hi, step, 0)

    def remote(src, dst, send, recv, **device):
        return pltpu.make_async_remote_copy(
            src_ref=src, dst_ref=dst, send_sem=send, recv_sem=recv,
            device_id=device, device_id_type=MESH,
        )

    def each_peer(body):
        def step(i, carry):
            body((me + 1 + i) % SP)
            return carry

        lax.fori_loop(0, SP - 1, step, 0)

    barrier = pltpu.get_barrier_semaphore()
    each_peer(
        lambda p: pl.semaphore_signal(barrier, inc=1, device_id={"sp": p}, device_id_type=MESH)
    )
    for off in range(1, Y):
        pl.semaphore_signal(
            barrier, inc=1, device_id={"tp": (t + 2 * off) % TP}, device_id_type=MESH
        )
    pl.semaphore_signal(barrier, inc=1, device_id={"tp": partner}, device_id_type=MESH)

    own_cols = pl.ds(pl.multiple_of(t * LANES, LANES), LANES)
    width = d_model // 2
    half_cols = pl.ds(pl.multiple_of(core * width, width), width)
    fetch = [
        pltpu.make_async_copy(src, dst, ins.at[k])
        for k, (src, dst) in enumerate(
            (
                (ids_h, ids), (wts_h, wts), (mix_h.at[:, own_cols], mix),
                (outg_h.at[:, own_cols], outg), (st_h, st), (wg_h, wg), (wu_h, wu), (wd_h, wd),
                (gbr_h, gbr), (dec_h, dec), (wp_h, wp),
                (mix_h.at[:, half_cols], mixh), (outg_h.at[:, half_cols], outh),
            )
        )
    ]
    for copy in fetch:
        copy.start()
    for copy in fetch[:4]:
        copy.wait()

    expert_io = lax.broadcasted_iota(jnp.int32, (SP, n), 0)
    hots = [(expert_io == ids[k : k + 1, :]).astype(F32) for k in range(2)]
    earlier = (
        lax.broadcasted_iota(jnp.int32, (n, n), 0) < lax.broadcasted_iota(jnp.int32, (n, n), 1)
    ).astype(F32).astype(BF16)
    before = dot((hots[0] + hots[1]).astype(BF16), earlier)
    row = lax.broadcasted_iota(jnp.int32, (slots, n), 0)
    kk = row >> (CAP.bit_length() - 1)
    zi = kk >> (X.bit_length() - 1)
    zz = (z + Z + ((zi + 1) >> 1) * (2 * (zi & 1) - 1)) & (Z - 1)
    xx = (x + (kk & (X - 1))) & (X - 1)
    slot_io = ((zz * X + xx) * CAP + (row & (CAP - 1))).astype(F32)
    picks = []
    for k in range(2):
        pos = jnp.sum(hots[k] * before, axis=0, keepdims=True)
        picks.append(slot_io == ids[k : k + 1, :].astype(F32) * float(CAP) + pos)
    onehot = (picks[0] | picks[1]).astype(F32).astype(BF16)
    onehot_s[...] = onehot
    weight = jnp.sum(
        jnp.where(picks[0], wts[0:1, :], 0.0) + jnp.where(picks[1], wts[1:2, :], 0.0),
        axis=1, keepdims=True,
    )
    weight_s[...] = weight + jnp.zeros((slots, LANES), F32)
    first = near * CAP

    def into(ref, begin, lo, hi, mix_ref, out_ref):
        pick = onehot_s[lo:hi, :]
        shape = ((hi - lo) // CAP, CAP, mix_ref.shape[1])
        end = begin + (hi - lo) // CAP
        ref[begin:end, 0:CAP, :] = dot(pick, mix_ref[...]).astype(BF16).reshape(shape)
        scaled = weight_s[lo:hi, 0:1] * dot(pick, out_ref[...])
        ref[begin:end, CAP : 2 * CAP, :] = scaled.astype(BF16).reshape(shape)

    into(disp, 0, first, slots, mix, outg)

    pl.semaphore_wait(barrier, SP - 1 + Y)

    def dispatch(k):
        return remote(disp.at[k], xc.at[t, k], s1.at[k], r1.at[k], sp=target(near + k))

    def dispatch_near(k):
        return remote(near_send.at[k], xd.at[core, k], n1.at[k], nr.at[core, k], sp=target(k))

    def across_near(k, half):
        return remote(xd.at[half, k], xd.at[half, k], n2.at[k], nr.at[half, k], tp=partner)

    each_block(0, far, lambda k: dispatch(k).start())
    for copy in fetch[11:]:
        copy.wait()
    into(near_send, 0, 0, first, mixh, outh)
    xd[core, 0] = near_send[0]
    across_near(0, core).start()
    for copy in fetch[4:11]:
        copy.wait()
    last_state = remote(
        st.at[pl.ds(n - 8, 8)], prev_b, vs.at[0], vr.at[0], sp=(me + 1) % SP
    )
    last_state.start()

    def arrived_1(g):
        lo, count = groups[g]
        each_block(lo, lo + count, lambda k: dispatch(k).wait_recv())

    def half_of(src, h):
        return xc.at[src, pl.ds(groups[h][0], groups[h][1])]

    def ring(src, h, way, step):
        dev = right if way == 0 else left
        return remote(half_of(src, h), half_of(src, h), rs.at[way, h, step], rr.at[src, h], tp=dev)

    def across(src, h):
        return remote(
            half_of(src, h), half_of(src, h), ds.at[src // 2, h], rr.at[src, h], tp=partner
        )

    acc_gu[...] = jnp.zeros_like(acc_gu)
    acc_h[...] = jnp.zeros_like(acc_h)

    def span(part):
        return (0, CAP) if part == 0 else (CAP, 2 * CAP)

    def pair_of(yy, part):
        lo, hi = span(part)
        return jnp.concatenate(
            [xc[2 * yy + k, :, lo:hi, :].reshape(far * CAP, LANES) for k in range(2)], axis=1
        )

    def near_rows(yy, part):
        lo, hi = span(part)
        at = yy % H * 2 * LANES
        return xd[yy // H, :, lo:hi, at : at + 2 * LANES].reshape(first, 2 * LANES)

    def forward_near(half):
        cols = pl.ds(pl.multiple_of(half * width, width), width)
        w_in = jnp.concatenate([wg[:, cols], wu[:, cols]], axis=0)
        rows_x = xd[half, :, 0:CAP, :].reshape(first, width)
        rows_c = xd[half, :, CAP : 2 * CAP, :].reshape(first, width)
        acc_gu[0:first] += dot(rows_x, w_in, ((1,), (1,)))
        acc_h[0:first] += dot(rows_c, wd[:, cols], ((1,), (1,)))

    def cols_of(yy):
        return pl.ds(pl.multiple_of(yy * 2 * LANES, 2 * LANES), 2 * LANES)

    def forward(yy):
        other = 2 * yy + 1 - core
        for h in range(len(groups)):
            across(other, h).wait_recv()
        cols = cols_of(yy)
        w_in = jnp.concatenate([wg[:, cols], wu[:, cols]], axis=0)
        acc_gu[first:slots] += dot(pair_of(yy, 0), w_in, ((1,), (1,)))
        acc_h[first:slots] += dot(pair_of(yy, 1), wd[:, cols], ((1,), (1,)))

    def reach(way, h):
        return H if way == h % 2 else H - 1

    begins = [0.0, 0.0, 3.5, 4.2, 5.0, 5.9][: len(groups)]
    events = sorted(
        (begins[h] + 4.4 * step, step, h) for h in range(len(groups)) for step in range(H + 1)
    )
    last_of = {step: max(e for e in events if e[1] == step) for step in range(H + 1)}
    for event in events:
        _, step, h = event
        if step == 0:
            arrived_1(h)
            for way in range(2):
                ring(t, h, way, 0).start()
            across(t, h).start()
        for way in range(2) if step else ():
            most = reach(way, h)
            if step > most:
                continue
            src = 2 * chip(-step if way == 0 else step) + core
            ring(src, h, way, step - 1).wait_recv()
            if step < most:
                ring(src, h, way, step).start()
            across(src, h).start()
        if event != last_of[step]:
            continue
        if step == 0:
            each_block(1, near, lambda k: dispatch_near(k).start())
            continue
        if step == H - 1:

            def pass_near(k):
                dispatch_near(k).wait_recv()
                across_near(k, core).start()

            each_block(1, near, pass_near)
            forward_near(core)
        forward(chip(step - 1))
        if step > 1:
            forward(chip(1 - step))
    each_block(0, near, lambda k: across_near(k, 1 - core).wait_recv())
    forward_near(1 - core)
    forward(chip(H))

    gate = acc_gu[:, 0:LANES]
    up = acc_gu[:, LANES : 2 * LANES]
    hg = acc_h[...]
    sig = jax.nn.sigmoid(gate)
    silu = gate * sig
    hidden = (silu * up).astype(BF16)
    up_grad = (hg * silu).astype(BF16)
    gate_grad = (hg * up * sig * (1.0 + gate * (1.0 - sig))).astype(BF16)
    grads = jnp.concatenate([gate_grad, up_grad], axis=1)

    def partial(off):
        yy = chip(off)
        cols = cols_of(yy)
        value = dot(grads, jnp.concatenate([wg[:, cols], wu[:, cols]], axis=0)).astype(BF16)
        pbuf[yy, 0] = value[:, 0:LANES]
        pbuf[yy, 1] = value[:, LANES : 2 * LANES]
        swap(yy).start()

    def swap(yy):
        return remote(pbuf.at[yy, 1 - core], precv.at[yy], ps.at[yy], pr.at[yy], tp=partner)

    rows = slots // 4

    def own_sum(off, h):
        yy = chip(off)
        part = pl.ds(h * rows, rows)
        return pbuf[yy, core, part, :].astype(F32) + precv[yy, part, :].astype(F32)

    def chain(way, h, step):
        dev = right if way == 0 else left
        return remote(
            sbuf.at[way, h, step], rbuf.at[way, h, step],
            cs.at[way, h, step], cr.at[way, h, step], tp=dev,
        )

    flows = ((1, 2), (1, 3), (0, 0), (0, 1), (0, 2), (0, 3), (1, 0), (1, 1))

    def length(way, h):
        return H if way == h // 2 else H - 1

    def sign(way):
        return 1 if way == 0 else -1

    partial(H)
    partial(H - 1)
    partial(1 - H)
    swap(chip(H)).wait_recv()
    for way, h in flows[:4]:
        sbuf[way, h, 0] = own_sum(H, h).astype(BF16)
        chain(way, h, 0).start()
    for way, h in flows[4:]:
        off = sign(way) * (H - 1)
        if h % 2 == 0:
            swap(chip(off)).wait_recv()
        sbuf[way, h, 0] = own_sum(off, h).astype(BF16)
        chain(way, h, 0).start()
    for m in range(H - 2, 0, -1):
        partial(m)
        partial(-m)
    partial(0)
    for m in range(H - 2, 0, -1):
        swap(chip(m)).wait_recv()
        swap(chip(-m)).wait_recv()
    swap(chip(0)).wait_recv()

    grads_t = grads.T
    hidden_t = hidden.T

    def all_rows(yy, part):
        return jnp.concatenate([near_rows(yy, part), pair_of(yy, part)], axis=0)

    def weight_grads(yy):
        cols = cols_of(yy)
        both = dot(grads_t, all_rows(yy, 0)).astype(BF16)
        o_gate[:, cols] = both[0:LANES]
        o_up[:, cols] = both[LANES : 2 * LANES]
        o_down[:, cols] = dot(hidden_t, all_rows(yy, 1)).astype(BF16)

    todo = list(range(Y))
    per_step = -(-Y // H)
    for s in range(1, H):
        for _ in range(per_step):
            if todo:
                weight_grads(todo.pop(0))
        for way, h in flows:
            most = length(way, h)
            if s >= most:
                continue
            off = sign(way) * (most - s)
            chain(way, h, s - 1).wait_recv()
            sbuf[way, h, s] = (rbuf[way, h, s - 1].astype(F32) + own_sum(off, h)).astype(BF16)
            chain(way, h, s).start()
    while todo:
        weight_grads(todo.pop(0))

    def give(k):
        return remote(fin.at[k], ret.at[k], fs.at[k], fr.at[k], sp=source(k))

    for h in (2, 3, 0, 1):
        total = own_sum(0, h)
        for way in range(2):
            step = length(way, h) - 1
            chain(way, h, step).wait_recv()
            total = total + rbuf[way, h, step].astype(F32)
        fin[pl.ds(h * quarter, quarter)] = total.astype(BF16).reshape(quarter, CAP, LANES)

        each_block(max(1, h * quarter), (h + 1) * quarter, lambda k: give(k).start())
    ret[0] = fin[0]

    onehot_t = onehot_s[...].T
    out_cols = outg[...].astype(F32)
    gated = (gbr[...].astype(F32) * st[...]).astype(BF16)
    prod = shift_up(dec[...], 1, 1.0)
    shifts = [1 << k for k in range((n - 1).bit_length())]
    prods = []
    for k in shifts:
        prods.append(prod)
        prod = prod * shift_up(prod, k, 1.0)

    each_block(1, SP, lambda k: give(k).wait_recv())
    routed = dot(onehot_t, ret[...].reshape(slots, LANES))
    mid_all[t] = (out_cols + routed).astype(BF16)

    def share(off):
        return remote(
            mid_all.at[t], mid_all.at[t], ms.at[off], mr.at[t], tp=(t + 2 * off) % TP
        )

    def pass_mid(src):
        return remote(mid_all.at[src], mid_all.at[src], mf.at[src // 2], mr.at[src], tp=partner)

    order = [off for m in range(1, H) for off in (m, -m)] + [H]
    pass_mid(t).start()
    for off in order:
        share(off % Y).start()

    block = d_model // SP

    def over_x(yy, j):
        return remote(
            gx_send.at[yy, j], gx_recv.at[yy, x], xs.at[yy, j], xr.at[yy, x], sp=z * X + j
        )

    def over_z(yy):
        return remote(gz_send.at[yy], gz_recv.at[z], zs.at[yy], zr.at[z], sp=yy * X + x)

    def x_peers(body):
        for j in range(1, X):
            body((x + j) % X)

    def project(yy):
        pass_mid(2 * yy + 1 - core).wait_recv()
        mid = jnp.concatenate([mid_all[2 * yy], mid_all[2 * yy + 1]], axis=1)
        part = dot(mid.T, gated).astype(BF16)
        gx_send[yy] = part.reshape(X, block, LANES)
        x_peers(lambda j: over_x(yy, j).start())
        return dot(mid, wp[cols_of(yy), :])

    def forward_proj(yy):
        total = gx_send[yy, x].astype(F32)
        for j in range(1, X):
            src = (x + j) % X
            remote(
                gx_send.at[yy, src], gx_recv.at[yy, src], xs.at[yy, src], xr.at[yy, src],
                sp=z * X + src,
            ).wait_recv()
            total = total + gx_recv[yy, src].astype(F32)
        gz_send[yy] = total.astype(BF16)

        @pl.when(yy != z)
        def _():
            over_z(yy).start()

    act = None
    queue = [0]
    behind = []
    for off in order:
        src = 2 * chip(off) + core
        remote(mid_all.at[src], mid_all.at[src], mf.at[0], mr.at[src], tp=partner).wait_recv()
        pass_mid(src).start()
        ready = queue.pop(0)
        term = project(chip(ready))
        act = term if act is None else act + term
        queue.append(off)
        behind.append(ready)
        if len(behind) > 2:
            forward_proj(chip(behind.pop(0)))
    for off in queue:
        act = act + project(chip(off))
    for off in behind:
        forward_proj(chip(off))

    states = st[...]
    o_branch[...] = (act * states).astype(BF16)
    grad = act * gbr[...].astype(F32)
    for k, a in zip(shifts, prods):
        grad = grad + a * shift_up(grad, k, 0.0)

    head = dec[0:1, :]
    car_send[0:1, :] = head * prod[0:1, :]
    car_send[1:2, :] = head * grad[0:1, :]

    def carry_to(p):
        return remote(car_send, car_recv.at[me], ks.at[p], kr.at[me], sp=p)

    each_peer(lambda p: carry_to(p).start())
    for off in queue:
        forward_proj(chip(off))
    car_recv[me] = car_send[...]
    each_peer(lambda p: remote(car_send, car_recv.at[p], ks.at[p], kr.at[p], sp=p).wait_recv())

    def enter(i, value):
        b = SP - 1 - i
        pair = car_recv[b]
        later = jnp.where(b > me, 1.0, 0.0)
        return later * (pair[1:2, :] + pair[0:1, :] * value) + (1.0 - later) * value

    entering = lax.fori_loop(0, SP - 1, enter, jnp.zeros((1, LANES), F32))
    drive = grad + prod * entering
    o_drive[...] = drive
    last_state.wait_recv()
    prior = jnp.where(me > 0, 1.0, 0.0) * prev_b[7:8, :]
    o_decay[...] = drive * jnp.concatenate([prior, states[: n - 1]], axis=0)

    def z_peers(body):
        def step(i, carry):
            body((z + 1 + i) % Y)
            return carry

        lax.fori_loop(0, Y - 1, step, 0)

    z_peers(
        lambda p: remote(
            gz_send.at[p], gz_recv.at[p], zs.at[p], zr.at[p], sp=p * X + x
        ).wait_recv()
    )
    total = gz_send[z].astype(F32)
    for i in range(1, Y):
        total = total + gz_recv[(z + i) % Y].astype(F32)
    o_proj[...] = total

    def drain(p):
        carry_to(p).wait_send()

    each_peer(drain)
    each_block(0, far, lambda k: dispatch(k).wait_send())
    each_block(1, near, lambda k: dispatch_near(k).wait_send())
    each_block(0, near, lambda k: across_near(k, core).wait_send())
    each_block(1, SP, lambda k: give(k).wait_send())
    last_state.wait_send()
    z_peers(lambda p: over_z(p).wait_send())
    for yy in range(Y):
        x_peers(lambda j: over_x(yy, j).wait_send())
    for way in range(2):
        for h in range(len(groups)):
            for step in range(reach(way, h)):
                ring(t, h, way, step).wait_send()
        for h in range(4):
            for step in range(length(way, h)):
                chain(way, h, step).wait_send()
    for yy in range(Y):
        for h in range(len(groups)):
            across(2 * yy + core, h).wait_send()
        swap(yy).wait_send()
        pass_mid(2 * yy + core).wait_send()
    for off in range(1, Y):
        share(off).wait_send()


def near_blocks(SP, X):
    return X


def ring_groups(far, X):
    rest = far - 2 * X
    parts = min(4, rest)
    sizes = [X, X] + [rest * (k + 1) // parts - rest * k // parts for k in range(parts)]
    return [(sum(sizes[:k]), sizes[k]) for k in range(len(sizes))]


def store(*refs):
    count = len(refs) // 2
    copies = [
        pltpu.make_async_copy(refs[k], refs[count + k], refs[-1].at[k]) for k in range(count)
    ]
    for copy in copies:
        copy.start()
    for copy in copies:
        copy.wait()


def local(
    mixer_out, out_grad, route_ids, route_weights, gate_branch, states, decay, w_proj,
    w_gate, w_up, w_down,
):
    n, d_model = mixer_out.shape
    SP = lax.axis_size("sp")
    TP = lax.axis_size("tp")
    Y, H = TP // 2, TP // 4
    CAP = min(n, 2 * route_ids.shape[1] * n // SP)
    slots = SP * CAP
    X = SP // Y
    near = near_blocks(SP, X)
    far = SP - near
    pieces = len(ring_groups(far, X))
    block = d_model // SP
    dma = pltpu.SemaphoreType.DMA
    big = jax.ShapeDtypeStruct((LANES, d_model), BF16)
    vmem = pl.BlockSpec(memory_space=pltpu.VMEM)
    outs = pl.pallas_call(
        functools.partial(kernel, (SP, SP // Y, TP, CAP)),
        out_shape=(
            big, big, big,
            jax.ShapeDtypeStruct((block, LANES), F32),
            jax.ShapeDtypeStruct((n, LANES), BF16),
            jax.ShapeDtypeStruct((n, LANES), F32),
            jax.ShapeDtypeStruct((n, LANES), F32),
        ),
        in_specs=[pl.BlockSpec(memory_space=pltpu.HBM)] * 11,
        out_specs=(vmem,) * 7,
        scratch_shapes=[
            pltpu.VMEM((2, n), jnp.int32),
            pltpu.VMEM((2, n), F32),
            pltpu.VMEM((n, LANES), BF16),
            pltpu.VMEM((n, LANES), BF16),
            pltpu.VMEM((n, LANES), BF16),
            pltpu.VMEM((n, LANES), F32),
            pltpu.VMEM((n, LANES), F32),
            pltpu.VMEM((d_model, LANES), BF16),
            pltpu.VMEM((LANES, d_model), BF16),
            pltpu.VMEM((LANES, d_model), BF16),
            pltpu.VMEM((LANES, d_model), BF16),
            pltpu.VMEM((n, d_model // 2), BF16),
            pltpu.VMEM((n, d_model // 2), BF16),
            pltpu.VMEM((slots, n), BF16),
            pltpu.VMEM((slots, LANES), F32),
            pltpu.VMEM((far, 2 * CAP, LANES), BF16),
            pltpu.VMEM((near, 2 * CAP, d_model // 2), BF16),
            pltpu.VMEM((2, near, 2 * CAP, d_model // 2), BF16),
            pltpu.VMEM((TP, far, 2 * CAP, LANES), BF16),
            pltpu.VMEM((slots, 2 * LANES), F32),
            pltpu.VMEM((slots, LANES), F32),
            pltpu.VMEM((Y, 2, slots, LANES), BF16),
            pltpu.VMEM((Y, slots, LANES), BF16),
            pltpu.VMEM((2, 4, H, slots // 4, LANES), BF16),
            pltpu.VMEM((2, 4, H, slots // 4, LANES), BF16),
            pltpu.VMEM((SP, CAP, LANES), BF16),
            pltpu.VMEM((SP, CAP, LANES), BF16),
            pltpu.VMEM((TP, n, LANES), BF16),
            pltpu.VMEM((Y, X, block, LANES), BF16),
            pltpu.VMEM((Y, X, block, LANES), BF16),
            pltpu.VMEM((Y, block, LANES), BF16),
            pltpu.VMEM((Y, block, LANES), BF16),
            pltpu.VMEM((2, LANES), F32),
            pltpu.VMEM((SP, 2, LANES), F32),
            pltpu.VMEM((8, LANES), F32),
            dma((13,)), dma((far,)), dma((far,)), dma((near,)), dma((near,)), dma((2, near)),
            dma((2, pieces, H)), dma((Y, pieces)), dma((TP, pieces)),
            dma((Y,)), dma((Y,)),
            dma((2, 4, H)), dma((2, 4, H)),
            dma((SP,)), dma((SP,)),
            dma((Y,)), dma((Y,)), dma((TP,)),
            dma((Y, X)), dma((Y, X)), dma((Y,)), dma((Y,)),
            dma((SP,)), dma((SP,)),
            dma((1,)), dma((1,)),
        ],
        compiler_params=pltpu.CompilerParams(
            collective_id=0, has_side_effects=True, vmem_limit_bytes=48 * 1024 * 1024
        ),
    )(*(pltpu.with_memory_space_constraint(a, pltpu.HBM) for a in (
        route_ids.T, route_weights.T, mixer_out, out_grad, gate_branch, states, decay, w_proj,
        w_gate[0], w_up[0], w_down[0],
    )))
    outs = pl.pallas_call(
        store,
        out_shape=tuple(jax.ShapeDtypeStruct(o.shape, o.dtype) for o in outs),
        in_specs=[vmem] * len(outs),
        out_specs=(pl.BlockSpec(memory_space=pltpu.HBM),) * len(outs),
        scratch_shapes=[dma((len(outs),))], compiler_params=pltpu.CompilerParams(vmem_limit_bytes=4194304),
    )(*outs)
    return (outs[0][None], outs[1][None], outs[2][None], *outs[3:])


def solution(mesh):
    placed = (
        P("sp", None),
        P("sp", None),
        P("sp", None),
        P("sp", None),
        P("sp", "tp"),
        P("sp", "tp"),
        P("sp", "tp"),
        P(None, "tp"),
        P("sp", "tp", None),
        P("sp", "tp", None),
        P("sp", "tp", None),
    )
    return jax.shard_map(
        local,
        mesh=mesh,
        in_specs=placed,
        out_specs=(
            P("sp", "tp", None),
            P("sp", "tp", None),
            P("sp", "tp", None),
            P("sp", "tp"),
            P("sp", "tp"),
            P("sp", "tp"),
            P("sp", "tp"),
        ),
        check_vma=False,
    )
```

```python
import functools
import jax
import jax.numpy as jnp
from jax import lax
from jax.experimental import pallas as pl
from jax.experimental.pallas import tpu as pltpu
from jax.sharding import PartitionSpec as P

F32 = jnp.float32
BF16 = jnp.bfloat16
LANES = 128
MESH = pl.DeviceIdType.MESH


def dot(a, b, contract=((1,), (0,))):
    return lax.dot_general(a, b, (contract, ((), ())), preferred_element_type=F32)


def shift_up(a, k, fill):
    pad = jnp.full((k, a.shape[1]), fill, a.dtype)
    return jnp.concatenate([a[k:], pad], axis=0)


def kernel(
    sizes,
    ids_h, wts_h, mix_h, outg_h, gbr_h, st_h, dec_h, wp_h, wg_h, wu_h, wd_h,
    o_gate, o_up, o_down, o_proj, o_branch, o_drive, o_decay,
    ids, wts, mix, outg, gbr, st, dec, wp, wg, wu, wd,
    mixh, outh, onehot_s, weight_s, disp, near_send, xd, xc, acc_gu, acc_h, pbuf, precv, sbuf, rbuf, fin, ret, mid_all,
    gx_send, gx_recv, gz_send, gz_recv, car_send, car_recv, prev_b,
    ins, s1, r1, n1, n2, nr, rs, ds, rr, ps, pr, cs, cr, fs, fr, ms, mf, mr, xs, xr, zs, zr, ks, kr, vs, vr,
):
    SP, X, TP, CAP = sizes
    Y = TP // 2
    H = Y // 2
    Z = SP // X
    near = near_blocks(SP, X)
    far = SP - near
    groups = ring_groups(far)
    quarter = SP // 4
    n = mix_h.shape[0]
    d_model = mix_h.shape[1]
    slots = SP * CAP
    me = lax.axis_index("sp")
    t = lax.axis_index("tp")
    y = t // 2
    core = t % 2
    partner = t + 1 - 2 * core
    right = (t + 2) % TP
    left = (t + TP - 2) % TP

    z = me // X
    x = me % X

    def chip(off):
        return (y + off + Y) % Y

    def moved(k, sign):
        zi = k // X
        dz = (zi + 1) // 2 * (2 * (zi % 2) - 1)
        return (z + sign * dz + Z) % Z * X + (x + sign * (k % X) + X) % X

    def target(k):
        return moved(k, 1)

    def source(k):
        return moved(k, -1)

    def each_block(lo, hi, body):
        def step(k, carry):
            body(k)
            return carry

        lax.fori_loop(lo, hi, step, 0)

    def remote(src, dst, send, recv, **device):
        return pltpu.make_async_remote_copy(
            src_ref=src, dst_ref=dst, send_sem=send, recv_sem=recv,
            device_id=device, device_id_type=MESH,
        )

    def each_peer(body):
        def step(i, carry):
            body((me + 1 + i) % SP)
            return carry

        lax.fori_loop(0, SP - 1, step, 0)

    barrier = pltpu.get_barrier_semaphore()
    each_peer(
        lambda p: pl.semaphore_signal(barrier, inc=1, device_id={"sp": p}, device_id_type=MESH)
    )
    for off in range(1, Y):
        pl.semaphore_signal(
            barrier, inc=1, device_id={"tp": (t + 2 * off) % TP}, device_id_type=MESH
        )
    pl.semaphore_signal(barrier, inc=1, device_id={"tp": partner}, device_id_type=MESH)

    own_cols = pl.ds(pl.multiple_of(t * LANES, LANES), LANES)
    width = d_model // 2
    half_cols = pl.ds(pl.multiple_of(core * width, width), width)
    fetch = [
        pltpu.make_async_copy(src, dst, ins.at[k])
        for k, (src, dst) in enumerate(
            (
                (ids_h, ids), (wts_h, wts), (mix_h.at[:, own_cols], mix),
                (outg_h.at[:, own_cols], outg), (st_h, st), (wg_h, wg), (wu_h, wu), (wd_h, wd),
                (gbr_h, gbr), (dec_h, dec), (wp_h, wp),
                (mix_h.at[:, half_cols], mixh), (outg_h.at[:, half_cols], outh),
            )
        )
    ]
    for copy in fetch:
        copy.start()
    for copy in fetch[:4]:
        copy.wait()

    expert_io = lax.broadcasted_iota(jnp.int32, (SP, n), 0)
    hots = [(expert_io == ids[k : k + 1, :]).astype(F32) for k in range(2)]
    earlier = (
        lax.broadcasted_iota(jnp.int32, (n, n), 0) < lax.broadcasted_iota(jnp.int32, (n, n), 1)
    ).astype(F32).astype(BF16)
    before = dot((hots[0] + hots[1]).astype(BF16), earlier)
    row = lax.broadcasted_iota(jnp.int32, (slots, n), 0)
    kk = row >> (CAP.bit_length() - 1)
    zi = kk >> (X.bit_length() - 1)
    zz = (z + Z + ((zi + 1) >> 1) * (2 * (zi & 1) - 1)) & (Z - 1)
    xx = (x + (kk & (X - 1))) & (X - 1)
    slot_io = ((zz * X + xx) * CAP + (row & (CAP - 1))).astype(F32)
    picks = []
    for k in range(2):
        pos = jnp.sum(hots[k] * before, axis=0, keepdims=True)
        picks.append(slot_io == ids[k : k + 1, :].astype(F32) * float(CAP) + pos)
    onehot = (picks[0] | picks[1]).astype(F32).astype(BF16)
    onehot_s[...] = onehot
    weight = jnp.sum(
        jnp.where(picks[0], wts[0:1, :], 0.0) + jnp.where(picks[1], wts[1:2, :], 0.0),
        axis=1, keepdims=True,
    )
    weight_s[...] = weight + jnp.zeros((slots, LANES), F32)
    first = near * CAP

    def into(ref, begin, lo, hi, mix_ref, out_ref):
        pick = onehot_s[lo:hi, :]
        shape = ((hi - lo) // CAP, CAP, mix_ref.shape[1])
        end = begin + (hi - lo) // CAP
        ref[begin:end, 0:CAP, :] = dot(pick, mix_ref[...]).astype(BF16).reshape(shape)
        scaled = weight_s[lo:hi, 0:1] * dot(pick, out_ref[...])
        ref[begin:end, CAP : 2 * CAP, :] = scaled.astype(BF16).reshape(shape)

    into(disp, 0, first, slots, mix, outg)

    pl.semaphore_wait(barrier, SP - 1 + Y)

    def dispatch(k):
        return remote(disp.at[k], xc.at[t, k], s1.at[k], r1.at[k], sp=target(near + k))

    def dispatch_near(k):
        return remote(near_send.at[k], xd.at[core, k], n1.at[k], nr.at[core, k], sp=target(k))

    def across_near(k, half):
        return remote(xd.at[half, k], xd.at[half, k], n2.at[k], nr.at[half, k], tp=partner)

    each_block(0, far, lambda k: dispatch(far - 1 - k).start())
    for copy in fetch[11:]:
        copy.wait()
    into(near_send, 0, 0, first, mixh, outh)
    xd[core, 0] = near_send[0]
    across_near(0, core).start()
    for copy in fetch[4:11]:
        copy.wait()
    last_state = remote(
        st.at[pl.ds(n - 8, 8)], prev_b, vs.at[0], vr.at[0], sp=(me + 1) % SP
    )
    last_state.start()

    def arrived_1(g):
        lo, count = groups[g]
        each_block(lo, lo + count, lambda k: dispatch(k).wait_recv())

    def half_of(src, h):
        return xc.at[src, pl.ds(groups[h][0], groups[h][1])]

    def ring(src, h, way, step):
        dev = right if way == 0 else left
        return remote(half_of(src, h), half_of(src, h), rs.at[way, h, step], rr.at[src, h], tp=dev)

    def across(src, h):
        return remote(
            half_of(src, h), half_of(src, h), ds.at[src // 2, h], rr.at[src, h], tp=partner
        )

    acc_gu[...] = jnp.zeros_like(acc_gu)
    acc_h[...] = jnp.zeros_like(acc_h)

    def span(part):
        return (0, CAP) if part == 0 else (CAP, 2 * CAP)

    def pair_of(yy, part):
        lo, hi = span(part)
        return jnp.concatenate(
            [xc[2 * yy + k, :, lo:hi, :].reshape(far * CAP, LANES) for k in range(2)], axis=1
        )

    def near_rows(yy, part):
        lo, hi = span(part)
        at = yy % H * 2 * LANES
        return xd[yy // H, :, lo:hi, at : at + 2 * LANES].reshape(first, 2 * LANES)

    def forward_near(half):
        cols = pl.ds(pl.multiple_of(half * width, width), width)
        w_in = jnp.concatenate([wg[:, cols], wu[:, cols]], axis=0)
        rows_x = xd[half, :, 0:CAP, :].reshape(first, width)
        rows_c = xd[half, :, CAP : 2 * CAP, :].reshape(first, width)
        acc_gu[0:first] += dot(rows_x, w_in, ((1,), (1,)))
        acc_h[0:first] += dot(rows_c, wd[:, cols], ((1,), (1,)))

    def cols_of(yy):
        return pl.ds(pl.multiple_of(yy * 2 * LANES, 2 * LANES), 2 * LANES)

    def forward(yy):
        other = 2 * yy + 1 - core
        for h in range(len(groups)):
            across(other, h).wait_recv()
        cols = cols_of(yy)
        w_in = jnp.concatenate([wg[:, cols], wu[:, cols]], axis=0)
        acc_gu[first:slots] += dot(pair_of(yy, 0), w_in, ((1,), (1,)))
        acc_h[first:slots] += dot(pair_of(yy, 1), wd[:, cols], ((1,), (1,)))

    def reach(way, h):
        return H if way == h % 2 else H - 1

    events = [(step, h) for step in range(H + 1) for h in range(len(groups))[::-1]]
    def other_near():
        each_block(0, near, lambda k: across_near(k, 1 - core).wait_recv())
        forward_near(1 - core)

    late = [lambda: forward(chip(H - 1)), lambda: forward(chip(1 - H)), other_near]
    for event in events:
        step, h = event
        if step == 0:
            arrived_1(h)
            for way in range(2):
                ring(t, h, way, 0).start()
            across(t, h).start()
        for way in range(2) if step else ():
            most = reach(way, h)
            if step > most:
                continue
            src = 2 * chip(-step if way == 0 else step) + core
            ring(src, h, way, step - 1).wait_recv()
            if step < most:
                ring(src, h, way, step).start()
            across(src, h).start()
        if step == H and late:
            late.pop(0)()
        if h:
            continue
        if step == 0:
            each_block(1, near, lambda k: dispatch_near(k).start())
            continue
        if step == H:
            continue
        forward(chip(step - 1))
        if step > 1:
            forward(chip(1 - step))
        if step == H - 1:

            def pass_near(k):
                dispatch_near(k).wait_recv()
                across_near(k, core).start()

            each_block(1, near, pass_near)
            forward_near(core)
    for job in late:
        job()
    forward(chip(H))

    gate = acc_gu[:, 0:LANES]
    up = acc_gu[:, LANES : 2 * LANES]
    hg = acc_h[...]
    sig = jax.nn.sigmoid(gate)
    silu = gate * sig
    hidden = (silu * up).astype(BF16)
    up_grad = (hg * silu).astype(BF16)
    gate_grad = (hg * up * sig * (1.0 + gate * (1.0 - sig))).astype(BF16)
    grads = jnp.concatenate([gate_grad, up_grad], axis=1)

    def partial(off):
        yy = chip(off)
        cols = cols_of(yy)
        value = dot(grads, jnp.concatenate([wg[:, cols], wu[:, cols]], axis=0)).astype(BF16)
        pbuf[yy, 0] = value[:, 0:LANES]
        pbuf[yy, 1] = value[:, LANES : 2 * LANES]
        swap(yy).start()

    def swap(yy):
        return remote(pbuf.at[yy, 1 - core], precv.at[yy], ps.at[yy], pr.at[yy], tp=partner)

    rows = slots // 4

    def own_sum(off, h):
        yy = chip(off)
        part = pl.ds(h * rows, rows)
        return pbuf[yy, core, part, :].astype(F32) + precv[yy, part, :].astype(F32)

    def chain(way, h, step):
        dev = right if way == 0 else left
        return remote(
            sbuf.at[way, h, step], rbuf.at[way, h, step],
            cs.at[way, h, step], cr.at[way, h, step], tp=dev,
        )

    flows = ((1, 2), (1, 3), (0, 0), (0, 1), (0, 2), (0, 3), (1, 0), (1, 1))

    def length(way, h):
        return H if way == h // 2 else H - 1

    def sign(way):
        return 1 if way == 0 else -1

    partial(H)
    partial(H - 1)
    partial(1 - H)
    swap(chip(H)).wait_recv()
    for way, h in flows[:4]:
        sbuf[way, h, 0] = own_sum(H, h).astype(BF16)
        chain(way, h, 0).start()
    for way, h in flows[4:]:
        off = sign(way) * (H - 1)
        if h % 2 == 0:
            swap(chip(off)).wait_recv()
        sbuf[way, h, 0] = own_sum(off, h).astype(BF16)
        chain(way, h, 0).start()
    for m in range(H - 2, 0, -1):
        partial(m)
        partial(-m)
    partial(0)
    for m in range(H - 2, 0, -1):
        swap(chip(m)).wait_recv()
        swap(chip(-m)).wait_recv()
    swap(chip(0)).wait_recv()

    grads_t = grads.T
    hidden_t = hidden.T

    def all_rows(yy, part):
        return jnp.concatenate([near_rows(yy, part), pair_of(yy, part)], axis=0)

    def weight_grads(yy):
        cols = cols_of(yy)
        both = dot(grads_t, all_rows(yy, 0)).astype(BF16)
        o_gate[:, cols] = both[0:LANES]
        o_up[:, cols] = both[LANES : 2 * LANES]
        o_down[:, cols] = dot(hidden_t, all_rows(yy, 1)).astype(BF16)

    todo = list(range(Y))
    per_step = -(-Y // H)
    for s in range(1, H):
        for _ in range(per_step):
            if todo:
                weight_grads(todo.pop(0))
        for way, h in flows:
            most = length(way, h)
            if s >= most:
                continue
            off = sign(way) * (most - s)
            chain(way, h, s - 1).wait_recv()
            sbuf[way, h, s] = (rbuf[way, h, s - 1].astype(F32) + own_sum(off, h)).astype(BF16)
            chain(way, h, s).start()
    while todo:
        weight_grads(todo.pop(0))

    def give(k):
        return remote(fin.at[k], ret.at[k], fs.at[0], fr.at[0], sp=source(k))

    for h in (2, 3, 0, 1):
        total = own_sum(0, h)
        for way in range(2):
            step = length(way, h) - 1
            chain(way, h, step).wait_recv()
            total = total + rbuf[way, h, step].astype(F32)
        fin[pl.ds(h * quarter, quarter)] = total.astype(BF16).reshape(quarter, CAP, LANES)

        each_block(max(1, h * quarter), (h + 1) * quarter, lambda k: give(k).start())
    ret[0] = fin[0]

    onehot_t = onehot_s[...].T
    out_cols = outg[...].astype(F32)
    gated = (gbr[...].astype(F32) * st[...]).astype(BF16)
    prod = shift_up(dec[...], 1, 1.0)
    shifts = [1 << k for k in range((n - 1).bit_length())]
    prods = []
    for k in shifts:
        prods.append(prod)
        prod = prod * shift_up(prod, k, 1.0)

    each_block(0, far, lambda k: dispatch(k).wait_send())
    each_block(1, near, lambda k: dispatch_near(k).wait_send())
    each_block(0, near, lambda k: across_near(k, core).wait_send())
    last_state.wait()
    for way in range(2):
        for h in range(len(groups)):
            for step in range(reach(way, h)):
                ring(t, h, way, step).wait_send()
        for h in range(4):
            for step in range(length(way, h)):
                chain(way, h, step).wait_send()
    for yy in range(Y):
        for h in range(len(groups)):
            across(2 * yy + core, h).wait_send()
        swap(yy).wait_send()
    rest = pl.ds(1, SP - 1)
    given = remote(fin.at[rest], ret.at[rest], fs.at[0], fr.at[0], sp=source(1))
    given.wait_recv()
    routed = dot(onehot_t, ret[...].reshape(slots, LANES))
    mid_all[t] = (out_cols + routed).astype(BF16)

    def share(off):
        return remote(
            mid_all.at[t], mid_all.at[t], ms.at[off], mr.at[t], tp=(t + 2 * off) % TP
        )

    def pass_mid(src):
        return remote(mid_all.at[src], mid_all.at[src], mf.at[src // 2], mr.at[src], tp=partner)

    order = [off for m in range(1, H) for off in (m, -m)] + [H]
    pass_mid(t).start()
    for off in order:
        share(off % Y).start()

    block = d_model // SP

    def over_x(yy, j):
        return remote(
            gx_send.at[yy, j], gx_recv.at[yy, x], xs.at[yy, j], xr.at[yy, x], sp=z * X + j
        )

    def over_z(yy):
        return remote(gz_send.at[yy], gz_recv.at[z], zs.at[yy], zr.at[z], sp=yy * X + x)

    def x_peers(body):
        for j in range(1, X):
            body((x + j) % X)

    def project(yy):
        pass_mid(2 * yy + 1 - core).wait_recv()
        mid = jnp.concatenate([mid_all[2 * yy], mid_all[2 * yy + 1]], axis=1)
        part = dot(mid.T, gated).astype(BF16)
        gx_send[yy] = part.reshape(X, block, LANES)
        x_peers(lambda j: over_x(yy, j).start())
        return dot(mid, wp[cols_of(yy), :])

    def forward_proj(yy):
        total = gx_send[yy, x].astype(F32)
        for j in range(1, X):
            src = (x + j) % X
            remote(
                gx_send.at[yy, src], gx_recv.at[yy, src], xs.at[yy, src], xr.at[yy, src],
                sp=z * X + src,
            ).wait_recv()
            total = total + gx_recv[yy, src].astype(F32)
        gz_send[yy] = total.astype(BF16)

        @pl.when(yy != z)
        def _():
            over_z(yy).start()

    act = None
    queue = [0]
    behind = []
    for off in order:
        src = 2 * chip(off) + core
        remote(mid_all.at[src], mid_all.at[src], mf.at[0], mr.at[src], tp=partner).wait_recv()
        pass_mid(src).start()
        ready = queue.pop(0)
        term = project(chip(ready))
        act = term if act is None else act + term
        queue.append(off)
        behind.append(ready)
        if len(behind) > 2:
            forward_proj(chip(behind.pop(0)))
    for off in queue:
        act = act + project(chip(off))

    states = st[...]
    o_branch[...] = (act * states).astype(BF16)
    grad = act * gbr[...].astype(F32)
    for k, a in zip(shifts, prods):
        grad = grad + a * shift_up(grad, k, 0.0)

    head = dec[0:1, :]
    car_send[0:1, :] = head * prod[0:1, :]
    car_send[1:2, :] = head * grad[0:1, :]

    def carry_to(p):
        return remote(car_send, car_recv.at[me], ks.at[0], kr.at[0], sp=p)

    each_peer(lambda p: carry_to(p).start())
    for off in behind + queue:
        forward_proj(chip(off))
    car_recv[me] = car_send[...]
    given.wait_send()
    for off in range(1, Y):
        share(off).wait_send()
    for yy in range(Y):
        pass_mid(2 * yy + core).wait_send()
        x_peers(lambda j: over_x(yy, j).wait_send())
    others = car_recv.at[pl.ds(0, SP - 1)]
    sent_carry = remote(others, others, ks.at[0], kr.at[0], sp=(me + 1) % SP)
    sent_carry.wait_recv()

    def enter(i, value):
        b = SP - 1 - i
        pair = car_recv[b]
        later = jnp.where(b > me, 1.0, 0.0)
        return later * (pair[1:2, :] + pair[0:1, :] * value) + (1.0 - later) * value

    entering = lax.fori_loop(0, SP - 1, enter, jnp.zeros((1, LANES), F32))
    drive = grad + prod * entering
    o_drive[...] = drive
    prior = jnp.where(me > 0, 1.0, 0.0) * prev_b[7:8, :]
    o_decay[...] = drive * jnp.concatenate([prior, states[: n - 1]], axis=0)

    def z_peers(body):
        def step(i, carry):
            body((z + 1 + i) % Y)
            return carry

        lax.fori_loop(0, Y - 1, step, 0)

    z_peers(
        lambda p: remote(
            gz_send.at[p], gz_recv.at[p], zs.at[p], zr.at[p], sp=p * X + x
        ).wait_recv()
    )
    total = gz_send[z].astype(F32)
    for i in range(1, Y):
        total = total + gz_recv[(z + i) % Y].astype(F32)
    o_proj[...] = total

    sent_carry.wait_send()
    z_peers(lambda p: over_z(p).wait_send())


def near_blocks(SP, X):
    return 3 * X


def ring_groups(far):
    parts = min(4, far)
    cuts = [far * k // parts for k in range(parts + 1)]
    return [(lo, hi - lo) for lo, hi in zip(cuts, cuts[1:])]


def store(*refs):
    count = len(refs) // 2
    copies = [
        pltpu.make_async_copy(refs[k], refs[count + k], refs[-1].at[k]) for k in range(count)
    ]
    for copy in copies:
        copy.start()
    for copy in copies:
        copy.wait()


def local(
    mixer_out, out_grad, route_ids, route_weights, gate_branch, states, decay, w_proj,
    w_gate, w_up, w_down,
):
    n, d_model = mixer_out.shape
    SP = lax.axis_size("sp")
    TP = lax.axis_size("tp")
    Y, H = TP // 2, TP // 4
    CAP = min(n, 2 * route_ids.shape[1] * n // SP)
    slots = SP * CAP
    X = SP // Y
    near = near_blocks(SP, X)
    far = SP - near
    pieces = len(ring_groups(far))
    block = d_model // SP
    dma = pltpu.SemaphoreType.DMA
    big = jax.ShapeDtypeStruct((LANES, d_model), BF16)
    vmem = pl.BlockSpec(memory_space=pltpu.VMEM)
    outs = pl.pallas_call(
        functools.partial(kernel, (SP, SP // Y, TP, CAP)),
        out_shape=(
            big, big, big,
            jax.ShapeDtypeStruct((block, LANES), F32),
            jax.ShapeDtypeStruct((n, LANES), BF16),
            jax.ShapeDtypeStruct((n, LANES), F32),
            jax.ShapeDtypeStruct((n, LANES), F32),
        ),
        in_specs=[pl.BlockSpec(memory_space=pltpu.HBM)] * 11,
        out_specs=(vmem,) * 7,
        scratch_shapes=[
            pltpu.VMEM((2, n), jnp.int32),
            pltpu.VMEM((2, n), F32),
            pltpu.VMEM((n, LANES), BF16),
            pltpu.VMEM((n, LANES), BF16),
            pltpu.VMEM((n, LANES), BF16),
            pltpu.VMEM((n, LANES), F32),
            pltpu.VMEM((n, LANES), F32),
            pltpu.VMEM((d_model, LANES), BF16),
            pltpu.VMEM((LANES, d_model), BF16),
            pltpu.VMEM((LANES, d_model), BF16),
            pltpu.VMEM((LANES, d_model), BF16),
            pltpu.VMEM((n, d_model // 2), BF16),
            pltpu.VMEM((n, d_model // 2), BF16),
            pltpu.VMEM((slots, n), BF16),
            pltpu.VMEM((slots, LANES), F32),
            pltpu.VMEM((far, 2 * CAP, LANES), BF16),
            pltpu.VMEM((near, 2 * CAP, d_model // 2), BF16),
            pltpu.VMEM((2, near, 2 * CAP, d_model // 2), BF16),
            pltpu.VMEM((TP, far, 2 * CAP, LANES), BF16),
            pltpu.VMEM((slots, 2 * LANES), F32),
            pltpu.VMEM((slots, LANES), F32),
            pltpu.VMEM((Y, 2, slots, LANES), BF16),
            pltpu.VMEM((Y, slots, LANES), BF16),
            pltpu.VMEM((2, 4, H, slots // 4, LANES), BF16),
            pltpu.VMEM((2, 4, H, slots // 4, LANES), BF16),
            pltpu.VMEM((SP, CAP, LANES), BF16),
            pltpu.VMEM((SP, CAP, LANES), BF16),
            pltpu.VMEM((TP, n, LANES), BF16),
            pltpu.VMEM((Y, X, block, LANES), BF16),
            pltpu.VMEM((Y, X, block, LANES), BF16),
            pltpu.VMEM((Y, block, LANES), BF16),
            pltpu.VMEM((Y, block, LANES), BF16),
            pltpu.VMEM((2, LANES), F32),
            pltpu.VMEM((SP, 2, LANES), F32),
            pltpu.VMEM((8, LANES), F32),
            dma((13,)), dma((far,)), dma((far,)), dma((near,)), dma((near,)), dma((2, near)),
            dma((2, pieces, H)), dma((Y, pieces)), dma((TP, pieces)),
            dma((Y,)), dma((Y,)),
            dma((2, 4, H)), dma((2, 4, H)),
            dma((1,)), dma((1,)),
            dma((Y,)), dma((Y,)), dma((TP,)),
            dma((Y, X)), dma((Y, X)), dma((Y,)), dma((Y,)),
            dma((1,)), dma((1,)),
            dma((1,)), dma((1,)),
        ],
        compiler_params=pltpu.CompilerParams(
            collective_id=0, has_side_effects=True, vmem_limit_bytes=48 * 1024 * 1024
        ),
    )(*(pltpu.with_memory_space_constraint(a, pltpu.HBM) for a in (
        route_ids.T, route_weights.T, mixer_out, out_grad, gate_branch, states, decay, w_proj,
        w_gate[0], w_up[0], w_down[0],
    )))
    outs = pl.pallas_call(
        store,
        out_shape=tuple(jax.ShapeDtypeStruct(o.shape, o.dtype) for o in outs),
        in_specs=[vmem] * len(outs),
        out_specs=(pl.BlockSpec(memory_space=pltpu.HBM),) * len(outs),
        scratch_shapes=[dma((len(outs),))], compiler_params=pltpu.CompilerParams(vmem_limit_bytes=4194304),
    )(*outs)
    return (outs[0][None], outs[1][None], outs[2][None], *outs[3:])


def solution(mesh):
    placed = (
        P("sp", None),
        P("sp", None),
        P("sp", None),
        P("sp", None),
        P("sp", "tp"),
        P("sp", "tp"),
        P("sp", "tp"),
        P(None, "tp"),
        P("sp", "tp", None),
        P("sp", "tp", None),
        P("sp", "tp", None),
    )
    return jax.shard_map(
        local,
        mesh=mesh,
        in_specs=placed,
        out_specs=(
            P("sp", "tp", None),
            P("sp", "tp", None),
            P("sp", "tp", None),
            P("sp", "tp"),
            P("sp", "tp"),
            P("sp", "tp"),
            P("sp", "tp"),
        ),
        check_vma=False,
    )
```

```python
import functools
import jax
import jax.numpy as jnp
from jax import lax
from jax.experimental import pallas as pl
from jax.experimental.pallas import tpu as pltpu
from jax.sharding import PartitionSpec as P

F32 = jnp.float32
BF16 = jnp.bfloat16
LANES = 128
MESH = pl.DeviceIdType.MESH


def dot(a, b, contract=((1,), (0,))):
    return lax.dot_general(a, b, (contract, ((), ())), preferred_element_type=F32)


def shift_up(a, k, fill):
    pad = jnp.full((k, a.shape[1]), fill, a.dtype)
    return jnp.concatenate([a[k:], pad], axis=0)


def kernel(
    sizes,
    ids_h, wts_h, mix_h, outg_h, gbr_h, st_h, dec_h, wp_h, wg_h, wu_h, wd_h,
    o_gate, o_up, o_down, o_proj, o_branch, o_drive, o_decay,
    ids, wts, mix, outg, gbr, st, dec, wp, wg, wu, wd,
    mixh, outh, onehot_s, weight_s, disp, near_send, xd, xc, acc_gu, acc_h, pbuf, precv, sbuf, rbuf, fin, ret, mid_all,
    gx_send, gx_recv, gz_send, gz_recv, car_send, car_recv, prev_b,
    ins, s1, r1, n1, n2, nr, rs, ds, rr, ps, pr, cs, cr, fs, fr, ms, mf, mr, xs, xr, zs, zr, ks, kr, vs, vr,
):
    SP, X, TP, CAP = sizes
    Y = TP // 2
    H = Y // 2
    Z = SP // X
    near = near_blocks(SP, X)
    far = SP - near
    groups = ring_groups(far)
    quarter = SP // 4
    n = mix_h.shape[0]
    d_model = mix_h.shape[1]
    slots = SP * CAP
    me = lax.axis_index("sp")
    t = lax.axis_index("tp")
    y = t // 2
    core = t % 2
    partner = t + 1 - 2 * core

    z = me // X
    x = me % X

    def chip(off):
        return (y + off + Y) % Y

    def other_core(off):
        return 2 * chip(off) + 1 - core

    right = other_core(1)
    left = other_core(-1)

    def lane(off):
        return core if off % 2 == 0 else 1 - core

    def moved(k, sign):
        zi = k // X
        dz = (zi + 1) // 2 * (2 * (zi % 2) - 1)
        return (z + sign * dz + Z) % Z * X + (x + sign * (k % X) + X) % X

    def target(k):
        return moved(k, 1)

    def source(k):
        return moved(k, -1)

    def each_block(lo, hi, body):
        def step(k, carry):
            body(k)
            return carry

        lax.fori_loop(lo, hi, step, 0)

    def each_peer(body):
        each_block(0, SP - 1, lambda i: body(target(SP - 1 - i)))

    def remote(src, dst, send, recv, **device):
        return pltpu.make_async_remote_copy(
            src_ref=src, dst_ref=dst, send_sem=send, recv_sem=recv,
            device_id=device, device_id_type=MESH,
        )

    own_cols = pl.ds(pl.multiple_of(t * LANES, LANES), LANES)
    width = d_model // 2
    half_cols = pl.ds(pl.multiple_of(core * width, width), width)
    fetch = [
        pltpu.make_async_copy(src, dst, ins.at[k])
        for k, (src, dst) in enumerate(
            (
                (ids_h, ids), (wts_h, wts), (mix_h.at[:, own_cols], mix),
                (outg_h.at[:, own_cols], outg), (st_h, st), (wg_h, wg), (wu_h, wu), (wd_h, wd),
                (gbr_h, gbr), (dec_h, dec), (wp_h, wp),
                (mix_h.at[:, half_cols], mixh), (outg_h.at[:, half_cols], outh),
            )
        )
    ]
    for copy in fetch:
        copy.start()

    barrier = pltpu.get_barrier_semaphore()
    each_peer(
        lambda p: pl.semaphore_signal(barrier, inc=1, device_id={"sp": p}, device_id_type=MESH)
    )
    for off in range(1, Y):
        pl.semaphore_signal(
            barrier, inc=1, device_id={"tp": other_core(off)}, device_id_type=MESH
        )
    pl.semaphore_signal(barrier, inc=1, device_id={"tp": partner}, device_id_type=MESH)

    for copy in fetch[:4]:
        copy.wait()

    expert_io = lax.broadcasted_iota(jnp.int32, (SP, n), 0)
    hots = [(expert_io == ids[k : k + 1, :]).astype(F32) for k in range(2)]
    earlier = (
        lax.broadcasted_iota(jnp.int32, (n, n), 0) < lax.broadcasted_iota(jnp.int32, (n, n), 1)
    ).astype(F32).astype(BF16)
    before = dot((hots[0] + hots[1]).astype(BF16), earlier)
    row = lax.broadcasted_iota(jnp.int32, (slots, n), 0)
    kk = row >> (CAP.bit_length() - 1)
    zi = kk >> (X.bit_length() - 1)
    zz = (z + Z + ((zi + 1) >> 1) * (2 * (zi & 1) - 1)) & (Z - 1)
    xx = (x + (kk & (X - 1))) & (X - 1)
    slot_io = ((zz * X + xx) * CAP + (row & (CAP - 1))).astype(F32)
    picks = []
    for k in range(2):
        pos = jnp.sum(hots[k] * before, axis=0, keepdims=True)
        picks.append(slot_io == ids[k : k + 1, :].astype(F32) * float(CAP) + pos)
    onehot = (picks[0] | picks[1]).astype(F32).astype(BF16)
    onehot_s[...] = onehot
    weight = jnp.sum(
        jnp.where(picks[0], wts[0:1, :], 0.0) + jnp.where(picks[1], wts[1:2, :], 0.0),
        axis=1, keepdims=True,
    )
    weight_s[...] = weight + jnp.zeros((slots, LANES), F32)
    first = near * CAP

    def into(ref, begin, lo, hi, mix_ref, out_ref):
        pick = onehot_s[lo:hi, :]
        shape = ((hi - lo) // CAP, CAP, mix_ref.shape[1])
        end = begin + (hi - lo) // CAP
        ref[begin:end, 0:CAP, :] = dot(pick, mix_ref[...]).astype(BF16).reshape(shape)
        scaled = weight_s[lo:hi, 0:1] * dot(pick, out_ref[...])
        ref[begin:end, CAP : 2 * CAP, :] = scaled.astype(BF16).reshape(shape)

    into(disp, 0, first, slots, mix, outg)

    pl.semaphore_wait(barrier, SP - 1 + Y)

    def dispatch(k):
        return remote(disp.at[k], xc.at[t, k], s1.at[k], r1.at[k], sp=target(near + k))

    def dispatch_near(k):
        return remote(near_send.at[k], xd.at[core, k], n1.at[k], nr.at[core, k], sp=target(k))

    def across_near(k, half):
        return remote(xd.at[half, k], xd.at[half, k], n2.at[k], nr.at[half, k], tp=partner)

    each_block(0, far, lambda k: dispatch(far - 1 - k).start())
    for copy in fetch[11:]:
        copy.wait()
    into(near_send, 0, 0, first, mixh, outh)
    xd[core, 0] = near_send[0]
    across_near(0, core).start()
    for copy in fetch[4:11]:
        copy.wait()
    last_state = remote(
        st.at[pl.ds(n - 8, 8)], prev_b, vs.at[0], vr.at[0], sp=(me + 1) % SP
    )
    last_state.start()

    def arrived_1(g):
        lo, count = groups[g]
        each_block(lo, lo + count, lambda k: dispatch(k).wait_recv())

    def half_of(src, h):
        return xc.at[src, pl.ds(groups[h][0], groups[h][1])]

    def ring(src, h, way, step):
        dev = right if way == 0 else left
        return remote(half_of(src, h), half_of(src, h), rs.at[way, h, step], rr.at[src, h], tp=dev)

    def across(src, h):
        return remote(
            half_of(src, h), half_of(src, h), ds.at[src // 2, h], rr.at[src, h], tp=partner
        )

    acc_gu[...] = jnp.zeros_like(acc_gu)
    acc_h[...] = jnp.zeros_like(acc_h)

    def span(part):
        return (0, CAP) if part == 0 else (CAP, 2 * CAP)

    def pair_of(yy, part):
        lo, hi = span(part)
        return jnp.concatenate(
            [xc[2 * yy + k, :, lo:hi, :].reshape(far * CAP, LANES) for k in range(2)], axis=1
        )

    def near_rows(yy, part):
        lo, hi = span(part)
        at = yy % H * 2 * LANES
        return xd[yy // H, :, lo:hi, at : at + 2 * LANES].reshape(first, 2 * LANES)

    def forward_near(half):
        cols = pl.ds(pl.multiple_of(half * width, width), width)
        w_in = jnp.concatenate([wg[:, cols], wu[:, cols]], axis=0)
        rows_x = xd[half, :, 0:CAP, :].reshape(first, width)
        rows_c = xd[half, :, CAP : 2 * CAP, :].reshape(first, width)
        acc_gu[0:first] += dot(rows_x, w_in, ((1,), (1,)))
        acc_h[0:first] += dot(rows_c, wd[:, cols], ((1,), (1,)))

    def cols_of(yy):
        return pl.ds(pl.multiple_of(yy * 2 * LANES, 2 * LANES), 2 * LANES)

    def forward(off):
        yy = chip(off)
        other = 2 * yy + 1 - lane(off)
        for h in range(len(groups)):
            across(other, h).wait_recv()
        cols = cols_of(yy)
        w_in = jnp.concatenate([wg[:, cols], wu[:, cols]], axis=0)
        acc_gu[first:slots] += dot(pair_of(yy, 0), w_in, ((1,), (1,)))
        acc_h[first:slots] += dot(pair_of(yy, 1), wd[:, cols], ((1,), (1,)))

    def reach(way, h):
        return H if way == h % 2 else H - 1

    events = [(step, h) for step in range(H + 1) for h in range(len(groups))[::-1]]
    def other_near():
        each_block(0, near, lambda k: across_near(k, 1 - core).wait_recv())
        forward_near(1 - core)

    late = [lambda: forward(H - 1), lambda: forward(1 - H), other_near]
    for event in events:
        step, h = event
        if step == 0:
            arrived_1(h)
            for way in range(2):
                ring(t, h, way, 0).start()
            across(t, h).start()
        for way in range(2) if step else ():
            most = reach(way, h)
            if step > most:
                continue
            src = 2 * chip(-step if way == 0 else step) + lane(step)
            ring(src, h, way, step - 1).wait_recv()
            if step < most:
                ring(src, h, way, step).start()
            across(src, h).start()
        if step == H and late:
            late.pop(0)()
        if h:
            continue
        if step == 0:
            each_block(1, near, lambda k: dispatch_near(k).start())
            continue
        if step == H:
            continue
        forward(step - 1)
        if step > 1:
            forward(1 - step)
        if step == H - 1:

            def pass_near(k):
                dispatch_near(k).wait_recv()
                across_near(k, core).start()

            each_block(1, near, pass_near)
            forward_near(core)
    for job in late:
        job()
    forward(H)

    gate = acc_gu[:, 0:LANES]
    up = acc_gu[:, LANES : 2 * LANES]
    hg = acc_h[...]
    sig = jax.nn.sigmoid(gate)
    silu = gate * sig
    hidden = (silu * up).astype(BF16)
    up_grad = (hg * silu).astype(BF16)
    gate_grad = (hg * up * sig * (1.0 + gate * (1.0 - sig))).astype(BF16)
    grads = jnp.concatenate([gate_grad, up_grad], axis=1)

    def partial(off):
        yy = chip(off)
        cols = cols_of(yy)
        value = dot(grads, jnp.concatenate([wg[:, cols], wu[:, cols]], axis=0)).astype(BF16)
        pbuf[yy, 0] = value[:, 0:LANES]
        pbuf[yy, 1] = value[:, LANES : 2 * LANES]
        swap(off).start()

    def swap(off):
        yy = chip(off)
        return remote(pbuf.at[yy, 1 - lane(off)], precv.at[yy], ps.at[yy], pr.at[yy], tp=partner)

    rows = slots // 4

    def own_sum(off, h):
        yy = chip(off)
        part = pl.ds(h * rows, rows)
        return pbuf[yy, lane(off), part, :].astype(F32) + precv[yy, part, :].astype(F32)

    def chain(way, h, step):
        dev = right if way == 0 else left
        return remote(
            sbuf.at[way, h, step], rbuf.at[way, h, step],
            cs.at[way, h, step], cr.at[way, h, step], tp=dev,
        )

    flows = ((1, 2), (1, 3), (0, 0), (0, 1), (0, 2), (0, 3), (1, 0), (1, 1))

    def length(way, h):
        return H if way == h // 2 else H - 1

    def sign(way):
        return 1 if way == 0 else -1

    partial(H)
    partial(H - 1)
    partial(1 - H)
    swap(H).wait_recv()
    for way, h in flows[:4]:
        sbuf[way, h, 0] = own_sum(H, h).astype(BF16)
        chain(way, h, 0).start()
    for way, h in flows[4:]:
        off = sign(way) * (H - 1)
        if h % 2 == 0:
            swap(off).wait_recv()
        sbuf[way, h, 0] = own_sum(off, h).astype(BF16)
        chain(way, h, 0).start()
    for m in range(H - 2, 0, -1):
        partial(m)
        partial(-m)
    partial(0)
    for m in range(H - 2, 0, -1):
        swap(m).wait_recv()
        swap(-m).wait_recv()
    swap(0).wait_recv()

    grads_t = grads.T
    hidden_t = hidden.T

    def all_rows(yy, part):
        return jnp.concatenate([near_rows(yy, part), pair_of(yy, part)], axis=0)

    def weight_grads(yy):
        cols = cols_of(yy)
        both = dot(grads_t, all_rows(yy, 0)).astype(BF16)
        o_gate[:, cols] = both[0:LANES]
        o_up[:, cols] = both[LANES : 2 * LANES]
        o_down[:, cols] = dot(hidden_t, all_rows(yy, 1)).astype(BF16)

    todo = list(range(Y))
    per_step = -(-Y // H)
    for s in range(1, H):
        for _ in range(per_step):
            if todo:
                weight_grads(todo.pop(0))
        for way, h in flows:
            most = length(way, h)
            if s >= most:
                continue
            off = sign(way) * (most - s)
            chain(way, h, s - 1).wait_recv()
            sbuf[way, h, s] = (rbuf[way, h, s - 1].astype(F32) + own_sum(off, h)).astype(BF16)
            chain(way, h, s).start()
    while todo:
        weight_grads(todo.pop(0))

    def give(k):
        return remote(fin.at[k], ret.at[k], fs.at[0], fr.at[0], sp=source(k))

    for h in (2, 3, 0, 1):
        total = own_sum(0, h)
        for way in range(2):
            step = length(way, h) - 1
            chain(way, h, step).wait_recv()
            total = total + rbuf[way, h, step].astype(F32)
        fin[pl.ds(h * quarter, quarter)] = total.astype(BF16).reshape(quarter, CAP, LANES)

        each_block(max(1, h * quarter), (h + 1) * quarter, lambda k: give(k).start())
    ret[0] = fin[0]

    onehot_t = onehot_s[...].T
    out_cols = outg[...].astype(F32)
    gated = (gbr[...].astype(F32) * st[...]).astype(BF16)
    prod = shift_up(dec[...], 1, 1.0)
    shifts = [1 << k for k in range((n - 1).bit_length())]
    prods = []
    for k in shifts:
        prods.append(prod)
        prod = prod * shift_up(prod, k, 1.0)

    each_block(0, far, lambda k: dispatch(k).wait_send())
    each_block(1, near, lambda k: dispatch_near(k).wait_send())
    each_block(0, near, lambda k: across_near(k, core).wait_send())
    last_state.wait()
    for way in range(2):
        for h in range(len(groups)):
            for step in range(reach(way, h)):
                ring(t, h, way, step).wait_send()
        for h in range(4):
            for step in range(length(way, h)):
                chain(way, h, step).wait_send()
    for yy in range(Y):
        for h in range(len(groups)):
            across(2 * yy + core, h).wait_send()
        swap(yy).wait_send()
    rest = pl.ds(1, SP - 1)
    given = remote(fin.at[rest], ret.at[rest], fs.at[0], fr.at[0], sp=source(1))
    given.wait_recv()
    routed = dot(onehot_t, ret[...].reshape(slots, LANES))
    mid_all[t] = (out_cols + routed).astype(BF16)

    def share(off):
        return remote(
            mid_all.at[t], mid_all.at[t], ms.at[off], mr.at[t], tp=other_core(off)
        )

    def pass_mid(src):
        return remote(mid_all.at[src], mid_all.at[src], mf.at[src // 2], mr.at[src], tp=partner)

    order = [off for m in range(1, H) for off in (m, -m)] + [H]
    pass_mid(t).start()
    for off in order:
        share(off % Y).start()

    block = d_model // SP

    def over_x(yy, j):
        return remote(
            gx_send.at[yy, j], gx_recv.at[yy, x], xs.at[yy, j], xr.at[yy, x], sp=z * X + j
        )

    def over_z(yy):
        return remote(gz_send.at[yy], gz_recv.at[z], zs.at[yy], zr.at[z], sp=yy * X + x)

    def x_peers(body):
        for j in range(1, X):
            body((x + j) % X)

    def project(off):
        yy = chip(off)
        pass_mid(2 * yy + (core if off else 1 - core)).wait_recv()
        mid = jnp.concatenate([mid_all[2 * yy], mid_all[2 * yy + 1]], axis=1)
        part = dot(mid.T, gated).astype(BF16)
        gx_send[yy] = part.reshape(X, block, LANES)
        x_peers(lambda j: over_x(yy, j).start())
        return dot(mid, wp[cols_of(yy), :])

    def forward_proj(yy):
        total = gx_send[yy, x].astype(F32)
        for j in range(1, X):
            src = (x + j) % X
            remote(
                gx_send.at[yy, src], gx_recv.at[yy, src], xs.at[yy, src], xr.at[yy, src],
                sp=z * X + src,
            ).wait_recv()
            total = total + gx_recv[yy, src].astype(F32)
        gz_send[yy] = total.astype(BF16)

        @pl.when(yy != z)
        def _():
            over_z(yy).start()

    act = None
    queue = [0]
    behind = []
    for off in order:
        src = other_core(off)
        remote(mid_all.at[src], mid_all.at[src], mf.at[0], mr.at[src], tp=partner).wait_recv()
        pass_mid(src).start()
        ready = queue.pop(0)
        term = project(ready)
        act = term if act is None else act + term
        queue.append(off)
        behind.append(ready)
    for off in queue:
        act = act + project(off)

    states = st[...]
    o_branch[...] = (act * states).astype(BF16)
    grad = act * gbr[...].astype(F32)
    for k, a in zip(shifts, prods):
        grad = grad + a * shift_up(grad, k, 0.0)

    head = dec[0:1, :]
    car_send[0:1, :] = head * prod[0:1, :]
    car_send[1:2, :] = head * grad[0:1, :]

    def carry_to(p):
        return remote(car_send, car_recv.at[me], ks.at[0], kr.at[0], sp=p)

    each_peer(lambda p: carry_to(p).start())
    for off in behind + queue:
        forward_proj(chip(off))
    car_recv[me] = car_send[...]
    given.wait_send()
    for off in range(1, Y):
        share(off).wait_send()
    for yy in range(Y):
        pass_mid(2 * yy + core).wait_send()
        x_peers(lambda j: over_x(yy, j).wait_send())
    others = car_recv.at[pl.ds(0, SP - 1)]
    sent_carry = remote(others, others, ks.at[0], kr.at[0], sp=(me + 1) % SP)
    sent_carry.wait_recv()

    def enter(i, value):
        b = SP - 1 - i
        pair = car_recv[b]
        later = jnp.where(b > me, 1.0, 0.0)
        return later * (pair[1:2, :] + pair[0:1, :] * value) + (1.0 - later) * value

    entering = lax.fori_loop(0, SP - 1, enter, jnp.zeros((1, LANES), F32))
    drive = grad + prod * entering
    o_drive[...] = drive
    prior = jnp.where(me > 0, 1.0, 0.0) * prev_b[7:8, :]
    o_decay[...] = drive * jnp.concatenate([prior, states[: n - 1]], axis=0)

    def z_peers(body):
        def step(i, carry):
            body((z + 1 + i) % Y)
            return carry

        lax.fori_loop(0, Y - 1, step, 0)

    z_peers(
        lambda p: remote(
            gz_send.at[p], gz_recv.at[p], zs.at[p], zr.at[p], sp=p * X + x
        ).wait_recv()
    )
    total = gz_send[z].astype(F32)
    for i in range(1, Y):
        total = total + gz_recv[(z + i) % Y].astype(F32)
    o_proj[...] = total

    sent_carry.wait_send()
    z_peers(lambda p: over_z(p).wait_send())


def near_blocks(SP, X):
    return 3 * X


def ring_groups(far):
    parts = min(4, far)
    cuts = [far * k // parts for k in range(parts + 1)]
    return [(lo, hi - lo) for lo, hi in zip(cuts, cuts[1:])]


def store(*refs):
    count = len(refs) // 2
    copies = [
        pltpu.make_async_copy(refs[k], refs[count + k], refs[-1].at[k]) for k in range(count)
    ]
    for copy in copies:
        copy.start()
    for copy in copies:
        copy.wait()


def local(
    mixer_out, out_grad, route_ids, route_weights, gate_branch, states, decay, w_proj,
    w_gate, w_up, w_down,
):
    n, d_model = mixer_out.shape
    SP = lax.axis_size("sp")
    TP = lax.axis_size("tp")
    Y, H = TP // 2, TP // 4
    CAP = min(n, 2 * route_ids.shape[1] * n // SP)
    slots = SP * CAP
    X = SP // Y
    near = near_blocks(SP, X)
    far = SP - near
    pieces = len(ring_groups(far))
    block = d_model // SP
    dma = pltpu.SemaphoreType.DMA
    big = jax.ShapeDtypeStruct((LANES, d_model), BF16)
    vmem = pl.BlockSpec(memory_space=pltpu.VMEM)
    outs = pl.pallas_call(
        functools.partial(kernel, (SP, SP // Y, TP, CAP)),
        out_shape=(
            big, big, big,
            jax.ShapeDtypeStruct((block, LANES), F32),
            jax.ShapeDtypeStruct((n, LANES), BF16),
            jax.ShapeDtypeStruct((n, LANES), F32),
            jax.ShapeDtypeStruct((n, LANES), F32),
        ),
        in_specs=[pl.BlockSpec(memory_space=pltpu.HBM)] * 11,
        out_specs=(vmem,) * 7,
        scratch_shapes=[
            pltpu.VMEM((2, n), jnp.int32),
            pltpu.VMEM((2, n), F32),
            pltpu.VMEM((n, LANES), BF16),
            pltpu.VMEM((n, LANES), BF16),
            pltpu.VMEM((n, LANES), BF16),
            pltpu.VMEM((n, LANES), F32),
            pltpu.VMEM((n, LANES), F32),
            pltpu.VMEM((d_model, LANES), BF16),
            pltpu.VMEM((LANES, d_model), BF16),
            pltpu.VMEM((LANES, d_model), BF16),
            pltpu.VMEM((LANES, d_model), BF16),
            pltpu.VMEM((n, d_model // 2), BF16),
            pltpu.VMEM((n, d_model // 2), BF16),
            pltpu.VMEM((slots, n), BF16),
            pltpu.VMEM((slots, LANES), F32),
            pltpu.VMEM((far, 2 * CAP, LANES), BF16),
            pltpu.VMEM((near, 2 * CAP, d_model // 2), BF16),
            pltpu.VMEM((2, near, 2 * CAP, d_model // 2), BF16),
            pltpu.VMEM((TP, far, 2 * CAP, LANES), BF16),
            pltpu.VMEM((slots, 2 * LANES), F32),
            pltpu.VMEM((slots, LANES), F32),
            pltpu.VMEM((Y, 2, slots, LANES), BF16),
            pltpu.VMEM((Y, slots, LANES), BF16),
            pltpu.VMEM((2, 4, H, slots // 4, LANES), BF16),
            pltpu.VMEM((2, 4, H, slots // 4, LANES), BF16),
            pltpu.VMEM((SP, CAP, LANES), BF16),
            pltpu.VMEM((SP, CAP, LANES), BF16),
            pltpu.VMEM((TP, n, LANES), BF16),
            pltpu.VMEM((Y, X, block, LANES), BF16),
            pltpu.VMEM((Y, X, block, LANES), BF16),
            pltpu.VMEM((Y, block, LANES), BF16),
            pltpu.VMEM((Y, block, LANES), BF16),
            pltpu.VMEM((2, LANES), F32),
            pltpu.VMEM((SP, 2, LANES), F32),
            pltpu.VMEM((8, LANES), F32),
            dma((13,)), dma((far,)), dma((far,)), dma((near,)), dma((near,)), dma((2, near)),
            dma((2, pieces, H)), dma((Y, pieces)), dma((TP, pieces)),
            dma((Y,)), dma((Y,)),
            dma((2, 4, H)), dma((2, 4, H)),
            dma((1,)), dma((1,)),
            dma((Y,)), dma((Y,)), dma((TP,)),
            dma((Y, X)), dma((Y, X)), dma((Y,)), dma((Y,)),
            dma((1,)), dma((1,)),
            dma((1,)), dma((1,)),
        ],
        compiler_params=pltpu.CompilerParams(
            collective_id=0, has_side_effects=True, vmem_limit_bytes=48 * 1024 * 1024
        ),
    )(*(pltpu.with_memory_space_constraint(a, pltpu.HBM) for a in (
        route_ids.T, route_weights.T, mixer_out, out_grad, gate_branch, states, decay, w_proj,
        w_gate[0], w_up[0], w_down[0],
    )))
    outs = pl.pallas_call(
        store,
        out_shape=tuple(jax.ShapeDtypeStruct(o.shape, o.dtype) for o in outs),
        in_specs=[vmem] * len(outs),
        out_specs=(pl.BlockSpec(memory_space=pltpu.HBM),) * len(outs),
        scratch_shapes=[dma((len(outs),))], compiler_params=pltpu.CompilerParams(vmem_limit_bytes=4194304),
    )(*outs)
    return (outs[0][None], outs[1][None], outs[2][None], *outs[3:])


def solution(mesh):
    placed = (
        P("sp", None),
        P("sp", None),
        P("sp", None),
        P("sp", None),
        P("sp", "tp"),
        P("sp", "tp"),
        P("sp", "tp"),
        P(None, "tp"),
        P("sp", "tp", None),
        P("sp", "tp", None),
        P("sp", "tp", None),
    )
    return jax.shard_map(
        local,
        mesh=mesh,
        in_specs=placed,
        out_specs=(
            P("sp", "tp", None),
            P("sp", "tp", None),
            P("sp", "tp", None),
            P("sp", "tp"),
            P("sp", "tp"),
            P("sp", "tp"),
            P("sp", "tp"),
        ),
        check_vma=False,
    )
```
